512 devices in a mesh: grp: 2 (over y), kv: 16 (over z), tp: 16 (over x, core).
Axes of the slice: x: 8, y: 2, z: 16, core: 2. Of those that a mesh axis runs over, the one named last changes fastest.
The devices are a block of a 8x16x16 slice.
Arguments:
- tokens: bfloat16 [256, 4096], P('grp', ('kv', 'tp')), parts along dimension 0, may hold values from -12 to 12
- gain_in: float32 [4096], P('kv'), may hold values from 0.1 to 1.9
- w_query: bfloat16 [4096, 1024], P('kv', 'tp'), may hold values from -0.09375 to 0.09375
- w_key: bfloat16 [4096, 1024], P('kv', 'tp'), may hold values from -0.09375 to 0.09375
- w_value: bfloat16 [4096, 2048], P('kv', 'tp'), may hold values from -0.09375 to 0.09375
- w_outgate: bfloat16 [4096, 2048], P('kv', 'tp'), may hold values from -0.09375 to 0.09375
- w_input_gate: bfloat16 [4096, 16], P('kv'), may hold values from -0.09375 to 0.09375
- w_forget_gate: bfloat16 [4096, 16], P('kv'), may hold values from -0.09375 to 0.09375
- bias_input: float32 [16], replicated, may hold values from -1 to 1
- bias_forget: float32 [16], replicated, may hold values from -1 to 4
- cell_state: float32 [256, 16, 64, 128], P(('grp', 'kv'), 'tp'), parts along dimension 0, may hold values from -6 to 6
- norm_state: float32 [256, 16, 64], P(('grp', 'kv'), 'tp'), parts along dimension 0, may hold values from -18 to 18
- max_state: float32 [256, 16], P(('grp', 'kv'), 'tp'), parts along dimension 0, may hold values from -1 to 2
- w_proj: bfloat16 [2048, 4096], P('tp', 'kv'), may hold values from -0.125 to 0.125
- gain_mid: float32 [4096], P('kv'), may hold values from 0.1 to 1.9
- w_up: bfloat16 [4096, 16384], P('kv', 'tp'), may hold values from -0.09375 to 0.09375
- w_down: bfloat16 [16384, 4096], P('tp', 'kv'), may hold values from -0.046875 to 0.046875
Outputs:
- mixed: bfloat16 [256, 4096], P('grp', ('kv', 'tp')), parts along dimension 0
- cell_new: float32 [256, 16, 64, 128], P(('grp', 'kv'), 'tp'), parts along dimension 0
- norm_new: float32 [256, 16, 64], P(('grp', 'kv'), 'tp'), parts along dimension 0
- max_new: float32 [256, 16], P(('grp', 'kv'), 'tp'), parts along dimension 0
The draws below stay inside these ranges and needn't reach their ends.
There are 2 independent parts, one for each index of `grp`. The reference program is written for one: setup_inputs(seed, part) draws one part's arguments, and reference() takes and returns one part's arrays. A program takes and returns all parts, laid end to end along the dimension named above; an argument that names none is the same for every part. Nothing has to cross between parts.
All inputs are finite; a program needn't handle non-finite values.
Results may differ from the reference program's by a relative error of at most 0.015.
Values may be sent and summed in bfloat16 or wider, within the bound.
No kernel may reach another device: no remote copies, remote signals or barrier semaphores. Data moves between devices by JAX's collectives and lax.ppermute only.
A program may use at most 64 MiB of HBM per device.

```python
import math
import jax
import jax.numpy as jnp
from jax import lax

D = 4096
NH = 16
DQK = 64
DV = 128
FF = 16384
BATCH = 128


def draw_tokens(key, part):
    key_scale = jax.random.fold_in(key, 11)
    key_base = jax.random.fold_in(key, 12)
    scales = jnp.exp(jax.random.uniform(key_scale, (16,), jnp.float32, math.log(0.3), math.log(3.0)))
    base = jnp.clip(jax.random.normal(key_base, (BATCH, D), jnp.float32), -4.0, 4.0)
    return (base * jnp.repeat(scales, D // 16)[None, :]).astype(jnp.bfloat16)


def block_levels(key, dims, pieces, smallest, top_value):
    level = 1.0
    for position, parts in pieces:
        draws = jax.random.uniform(jax.random.fold_in(jax.random.fold_in(key, 6), position), (parts,), jnp.float32, smallest / len(pieces), top_value / len(pieces))
        level = level * jnp.repeat(jnp.exp(draws), dims[position] // parts).reshape((-1,) + (1,) * (len(dims) - 1 - position))
    return level


def scatter_about(rng, extent, spread, limit, split=(), dtype=jnp.bfloat16):
    gain = block_levels(rng, extent, split, -0.22, 0.18) if split else 1.0
    array = jax.random.normal(rng, extent, jnp.float32) * spread * gain
    return jnp.minimum(jnp.maximum(array, -limit), limit).astype(dtype)


def setup_inputs(seed: int = 0, part: int = 0) -> dict:
    streams_of = jax.random.split(jax.random.key(seed), 18)
    own_keys = jax.random.split(jax.random.fold_in(streams_of[17], part), 18)
    return {
        "tokens": draw_tokens(jax.random.fold_in(jax.random.fold_in(streams_of[17], part), 71), part),
        "gain_in": jnp.clip(1.0 + 0.18 * jax.random.normal(streams_of[1], (D,), jnp.float32), 0.1, 1.9),
        "w_query": scatter_about(streams_of[2], (D, NH * DQK), D ** -0.5, 0.09375, ((0, 16), (1, 16))),
        "w_key": scatter_about(streams_of[3], (D, NH * DQK), D ** -0.5, 0.09375, ((0, 16), (1, 16))),
        "w_value": scatter_about(streams_of[4], (D, NH * DV), D ** -0.5, 0.09375, ((0, 16), (1, 16))),
        "w_outgate": scatter_about(streams_of[5], (D, NH * DV), D ** -0.5, 0.09375, ((0, 16), (1, 16))),
        "w_input_gate": scatter_about(streams_of[6], (D, NH), D ** -0.5, 0.09375, ((0, 16),)),
        "w_forget_gate": scatter_about(streams_of[7], (D, NH), D ** -0.5, 0.09375, ((0, 16),)),
        "bias_input": jnp.clip(jax.random.uniform(streams_of[8], (NH,), jnp.float32, -1.0, 1.0), -1.0, 1.0),
        "bias_forget": jnp.clip(jax.random.uniform(streams_of[9], (NH,), jnp.float32, -1.0, 4.0), -1.0, 4.0),
        "cell_state": scatter_about(own_keys[10], (BATCH, NH, DQK, DV), 1.0, 6.0, ((0, 16), (1, 16)), jnp.float32),
        "norm_state": scatter_about(own_keys[11], (BATCH, NH, DQK), 3.0, 18.0, ((0, 16), (1, 16)), jnp.float32),
        "max_state": jnp.clip(-1.0 + 3.0 * jax.random.uniform(own_keys[12], (BATCH, NH), jnp.float32) ** block_levels(own_keys[12], (BATCH, NH), ((0, 16), (1, 16)), -0.2, 0.2), -1.0, 2.0),
        "w_proj": scatter_about(streams_of[13], (NH * DV, D), (NH * DV) ** -0.5, 0.125, ((0, 16), (1, 16))),
        "gain_mid": jnp.clip(1.0 + 0.18 * jax.random.normal(streams_of[14], (D,), jnp.float32), 0.1, 1.9),
        "w_up": scatter_about(streams_of[15], (D, FF), D ** -0.5, 0.09375, ((0, 16), (1, 16))),
        "w_down": scatter_about(streams_of[16], (FF, D), FF ** -0.5, 0.046875, ((0, 16), (1, 16))),
    }


EPSILON = 1e-06

def memory_step(query, keys, values, outgate, log_input, log_forget, cell_state, norm_state, max_state):
    max_new = jnp.maximum(log_forget + max_state, log_input)
    keep = jnp.exp(log_forget + max_state - max_new)
    write = jnp.exp(log_input - max_new)
    cell_new = keep[..., None, None] * cell_state + (write[..., None] * keys)[..., :, None] * values[..., None, :]
    norm_new = keep[..., None] * norm_state + write[..., None] * keys
    numer = jnp.einsum('shk,shkv->shv', query, cell_new, precision=lax.Precision.HIGHEST)
    denom = jnp.maximum(jnp.abs(lax.optimization_barrier(jnp.sum(query * norm_new, axis=-1))), jnp.exp(-max_new))
    heads = (jax.nn.sigmoid(outgate) * numer / denom[..., None]).astype(jnp.bfloat16)
    return (heads, cell_new, norm_new, max_new)

def reference(tokens, gain_in, w_query, w_key, w_value, w_outgate, w_input_gate, w_forget_gate, bias_input, bias_forget, cell_state, norm_state, max_state, w_proj, gain_mid, w_up, w_down):
    rows = tokens.shape[0]
    widef = tokens.astype(jnp.float32)
    scale_in = lax.rsqrt(lax.optimization_barrier(jnp.sum(widef * widef, axis=1)) / D + EPSILON)
    normed = (widef * gain_in).astype(jnp.bfloat16)

    def project(weight):
        return jnp.dot(normed, weight, preferred_element_type=jnp.float32) * scale_in[:, None]
    query = project(w_query).reshape(rows, NH, DQK) * DQK ** (-0.5)
    keys = project(w_key).reshape(rows, NH, DQK)
    values = project(w_value).reshape(rows, NH, DV)
    outgate = project(w_outgate).reshape(rows, NH, DV)
    log_input = project(w_input_gate) + bias_input
    log_forget = jax.nn.log_sigmoid(project(w_forget_gate) + bias_forget)
    heads, cell_new, norm_new, max_new = memory_step(query, keys, values, outgate, log_input, log_forget, cell_state, norm_state, max_state)
    branch = jnp.dot(heads.reshape(rows, NH * DV), w_proj, preferred_element_type=jnp.float32)
    middle = (widef + branch).astype(jnp.bfloat16)
    midf = middle.astype(jnp.float32)
    scale_mid = lax.rsqrt(lax.optimization_barrier(jnp.sum(midf * midf, axis=1)) / D + EPSILON)
    normed_mid = (midf * gain_mid).astype(jnp.bfloat16)
    upward = jnp.dot(normed_mid, w_up, preferred_element_type=jnp.float32) * scale_mid[:, None]
    hidden = jnp.square(jax.nn.relu(upward)).astype(jnp.bfloat16)
    down = jnp.dot(hidden, w_down, preferred_element_type=jnp.float32)
    mixed = (midf + down).astype(jnp.bfloat16)
    return (mixed, cell_new, norm_new, max_new)
```

```python
import jax
import jax.numpy as jnp
from jax import lax
from jax.sharding import PartitionSpec as P

EPSILON = 1e-06
LANES = 128


def exchange(tiles, axis):
    return lax.all_to_all(tiles, axis, split_axis=0, concat_axis=0, tiled=True)


def spread(value, axis):
    return exchange(jnp.broadcast_to(value, (lax.axis_size(axis), *value.shape)), axis)


def contract(left, right, left_dim, right_dim):
    dims = (((left_dim,), (right_dim,)), ((), ()))
    return lax.dot_general(left, right, dims, preferred_element_type=jnp.float32)


def two_parts(value):
    high = lax.reduce_precision(value, 8, 7)
    return high, lax.reduce_precision(value - high, 8, 7)


def on_device(
    tokens,
    gain_in,
    w_query,
    w_key,
    w_value,
    w_outgate,
    w_input_gate,
    w_forget_gate,
    bias_input,
    bias_forget,
    cell_state,
    norm_state,
    max_state,
    w_proj,
    gain_mid,
    w_up,
    w_down,
):
    seqs, own_columns = tokens.shape
    key_dim, value_dim = cell_state.shape[2:]
    tp, kv = lax.axis_size("tp"), lax.axis_size("kv")
    rows = gain_in.shape[0]
    width = rows * kv
    head = lax.axis_index("tp")
    own = seqs // kv
    main = 2 * key_dim + 2 * value_dim

    own_tokens = tokens.T
    wide = spread(own_tokens, "tp").reshape(rows, seqs).astype(jnp.float32)
    normed = (wide * gain_in[:, None]).astype(jnp.bfloat16)
    squares = jnp.sum(wide * wide, axis=0)

    gate_in = lax.dynamic_slice_in_dim(w_input_gate, head, 1, 1)
    gate_forget = lax.dynamic_slice_in_dim(w_forget_gate, head, 1, 1)
    blank = jnp.zeros((rows, 1), jnp.bfloat16)
    rest = jnp.zeros((rows, LANES - 6), jnp.bfloat16)
    weights = jnp.concatenate(
        [w_query, w_key, w_value, w_outgate]
        + [gate_in, gate_forget, blank, gate_in, gate_forget, blank, rest],
        axis=1,
    )
    terms = contract(normed, weights, 0, 0)
    lane = lax.broadcasted_iota(jnp.int32, (seqs, LANES), 1)
    extra = jnp.where((lane == 2) | (lane == 5), squares[:, None], terms[:, main:])
    high, low = two_parts(extra)
    terms = jnp.concatenate([terms[:, :main], jnp.where(lane < 3, high, low)], axis=1)
    terms = exchange(terms.astype(jnp.bfloat16).reshape(kv, own, -1), "kv")
    terms = jnp.sum(terms.astype(jnp.float32), axis=0)
    extra = terms[:, main : main + 3] + terms[:, main + 3 : main + 6]
    scale = lax.rsqrt(extra[:, 2:3] / width + EPSILON)
    query = terms[:, :key_dim] * (scale * key_dim ** (-0.5))
    keys = terms[:, key_dim : 2 * key_dim] * scale
    values = terms[:, 2 * key_dim : 2 * key_dim + value_dim] * scale
    outgate = terms[:, 2 * key_dim + value_dim : main] * scale

    cell, norm = cell_state[:, 0], norm_state[:, 0]
    log_input = extra[:, 0:1] * scale + lax.dynamic_slice_in_dim(bias_input, head, 1, 0)
    log_forget = jax.nn.log_sigmoid(
        extra[:, 1:2] * scale + lax.dynamic_slice_in_dim(bias_forget, head, 1, 0)
    )
    max_new = jnp.maximum(log_forget + max_state, log_input)
    keep = jnp.exp(log_forget + max_state - max_new)
    write = jnp.exp(log_input - max_new)
    written = write * keys
    norm_new = keep * norm + written
    cell_new = keep[..., None] * cell + written[:, :, None] * values[:, None, :]
    numer = jnp.sum(query[:, :, None] * cell_new, axis=1)
    denom = jnp.maximum(
        jnp.abs(jnp.sum(query * norm_new, axis=1, keepdims=True)), jnp.exp(-max_new)
    )
    heads = (jax.nn.sigmoid(outgate) * numer / denom).astype(jnp.bfloat16)

    heads = spread(heads, "kv").reshape(seqs, value_dim)
    branch = contract(w_proj, heads, 0, 1).astype(jnp.bfloat16)
    branch = exchange(branch.reshape(tp, own_columns, seqs), "tp")
    own_middle = own_tokens.astype(jnp.float32) + jnp.sum(branch.astype(jnp.float32), axis=0)
    own_middle = own_middle.astype(jnp.bfloat16)
    middle = spread(own_middle, "tp").reshape(rows, seqs).astype(jnp.float32)
    mid_squares = jnp.sum(middle * middle, axis=0)
    normed_mid = (middle * gain_mid[:, None]).astype(jnp.bfloat16)
    upward = contract(normed_mid, w_up, 0, 0)
    upward = jnp.concatenate([upward, mid_squares[:, None]], axis=1).astype(jnp.bfloat16)
    upward = exchange(upward.reshape(kv, own, -1), "kv")
    upward = jnp.sum(upward.astype(jnp.float32), axis=0)
    scale_mid = lax.rsqrt(upward[:, -1:] / width + EPSILON)
    hidden = jnp.square(jax.nn.relu(upward[:, :-1] * scale_mid)).astype(jnp.bfloat16)

    hidden = lax.all_gather(hidden, "kv", axis=0, tiled=True)
    down = contract(w_down, hidden, 0, 1).astype(jnp.bfloat16)
    down = exchange(down.reshape(tp, own_columns, seqs), "tp")
    mixed = own_middle.astype(jnp.float32) + jnp.sum(down.astype(jnp.float32), axis=0)
    mixed = mixed.astype(jnp.bfloat16).T
    return (mixed, cell_new[:, None], norm_new[:, None], max_new)


def solution(mesh):
    in_specs = (
        P("grp", ("kv", "tp")),
        P("kv"),
        P("kv", "tp"),
        P("kv", "tp"),
        P("kv", "tp"),
        P("kv", "tp"),
        P("kv", None),
        P("kv", None),
        P(),
        P(),
        P(("grp", "kv"), "tp", None, None),
        P(("grp", "kv"), "tp", None),
        P(("grp", "kv"), "tp"),
        P("tp", "kv"),
        P("kv"),
        P("kv", "tp"),
        P("tp", "kv"),
    )
    out_specs = (
        P("grp", ("kv", "tp")),
        P(("grp", "kv"), "tp", None, None),
        P(("grp", "kv"), "tp", None),
        P(("grp", "kv"), "tp"),
    )
    return jax.shard_map(
        on_device, mesh=mesh, in_specs=in_specs, out_specs=out_specs, check_vma=False
    )
```

```python
import functools

import jax
import jax.numpy as jnp
from jax import lax
from jax.experimental import pallas as pl
from jax.experimental.pallas import tpu as pltpu
from jax.sharding import PartitionSpec as P

EPSILON = 1e-06
LANES = 128


def exchange(tiles, axis):
    return lax.all_to_all(tiles, axis, split_axis=0, concat_axis=0, tiled=True)


def spread(value, axis):
    return exchange(jnp.broadcast_to(value, (lax.axis_size(axis), *value.shape)), axis)


def contract(left, right, left_dim, right_dim):
    dims = (((left_dim,), (right_dim,)), ((), ()))
    return lax.dot_general(left, right, dims, preferred_element_type=jnp.float32)


def two_parts(value):
    high = value.astype(jnp.bfloat16).astype(jnp.float32)
    return high, (value - high).astype(jnp.bfloat16).astype(jnp.float32)


def project_body(tokens, aux, wq, wk, wv, wo, wi, wf, out):
    gain, pick = aux[0:1], aux[1:2, : wi.shape[0]]
    wide = tokens[...].reshape(-1, tokens.shape[-1]).astype(jnp.float32).T
    squares = jnp.sum(wide * wide, axis=1, keepdims=True)
    normed = (wide * gain).astype(jnp.bfloat16)
    query = contract(normed, wq[...], 1, 1)
    keys = contract(normed, wk[...], 1, 1)
    values = contract(normed, wv[...], 1, 0)
    outgate = contract(normed, wo[...], 1, 0)
    gate_in = jnp.sum(contract(normed, wi[...], 1, 1) * pick, axis=1, keepdims=True)
    gate_forget = jnp.sum(contract(normed, wf[...], 1, 1) * pick, axis=1, keepdims=True)
    lane = lax.broadcasted_iota(jnp.int32, (wide.shape[0], LANES), 1)
    extra = jnp.zeros((wide.shape[0], LANES), jnp.float32)
    for place, value in enumerate((gate_in, gate_forget, squares)):
        high, low = two_parts(value)
        extra = jnp.where(lane == place, high, extra)
        extra = jnp.where(lane == place + 3, low, extra)
    both = jnp.concatenate([query, keys], axis=1)
    peers, own, _ = out.shape
    at = 0
    for piece in (both, values, outgate, extra):
        piece = piece.astype(jnp.bfloat16)
        for peer in range(peers):
            out[peer, :, at : at + LANES] = piece[peer * own : (peer + 1) * own]
        at += LANES


def memory_body(
    width, tiles, cell, aux,
    heads, cell_out, norm_out, top_out, cell_new, norm_buf, top_buf, sems,
):
    own, key_dim, value_dim = cell.shape
    terms = jnp.sum(tiles[...].astype(jnp.float32), axis=0)
    extra = terms[:, 3 * LANES :]
    extra = extra[:, 0:3] + extra[:, 3:6]
    scale = lax.rsqrt(extra[:, 2:3] / width + EPSILON)
    side = aux[...]
    norm, top = side[:, :key_dim], side[:, key_dim : key_dim + 1]
    log_input = extra[:, 0:1] * scale + side[:, key_dim + 1 : key_dim + 2]
    forget = extra[:, 1:2] * scale + side[:, key_dim + 2 : key_dim + 3]
    log_forget = jnp.minimum(forget, 0.0) - jnp.log1p(jnp.exp(-jnp.abs(forget)))
    log_keep = log_forget + top
    max_new = jnp.maximum(log_keep, log_input)
    keep = jnp.exp(log_keep - max_new)
    write = jnp.exp(log_input - max_new)
    top_buf[...] = jnp.broadcast_to(max_new, (own, LANES)).T[0:1]
    lane = lax.broadcasted_iota(jnp.int32, (own, LANES), 1)
    is_query = lane < key_dim
    both = terms[:, :LANES] * jnp.where(is_query, scale * key_dim ** (-0.5), scale * write)
    values = terms[:, LANES : 2 * LANES] * scale
    outgate = terms[:, 2 * LANES : 3 * LANES] * scale
    turned = jnp.concatenate([both] * (LANES // own), axis=0).T
    norm_new = keep * norm + both[:, key_dim:]
    norm_buf[...] = norm_new
    copies = [
        pltpu.make_async_copy(top_buf, top_out, sems.at[own]),
        pltpu.make_async_copy(norm_buf, norm_out, sems.at[own + 1]),
    ]
    for copy in copies:
        copy.start()
    rows = []
    for s in range(own):
        fresh = keep[s : s + 1] * cell[s] + turned[key_dim:, s : s + 1] * values[s : s + 1]
        cell_new[s] = fresh
        copies.append(pltpu.make_async_copy(cell_new.at[s], cell_out.at[s], sems.at[s]))
        copies[-1].start()
        rows.append(jnp.sum(turned[:key_dim, s : s + 1] * fresh, axis=0, keepdims=True))
    numer = jnp.concatenate(rows, axis=0)
    dot = jnp.sum(both[:, :key_dim] * norm_new, axis=1, keepdims=True)
    denom = jnp.maximum(jnp.abs(dot), jnp.exp(-max_new))
    done = (numer * (1.0 / (1.0 + jnp.exp(-outgate))) / denom).astype(jnp.bfloat16)
    for peer in range(heads.shape[0]):
        heads[peer] = done
    for copy in copies:
        copy.wait()


def on_chip(*arrays):
    return [pltpu.with_memory_space_constraint(a, pltpu.VMEM) for a in arrays]


def project(tokens, aux, weights, peers):
    seqs = tokens.shape[-1]
    return pl.pallas_call(
        project_body,
        out_shape=pltpu.VMEM((peers, seqs // peers, 4 * LANES), jnp.bfloat16),
        name="project",
    )(*on_chip(tokens, aux, *weights))


def memory_step(tiles, cell, aux, width):
    peers, own, _ = tiles.shape
    _, key_dim, value_dim = cell.shape
    vmem = pl.BlockSpec(memory_space=pltpu.VMEM)
    hbm = pl.BlockSpec(memory_space=pl.ANY)
    return pl.pallas_call(
        functools.partial(memory_body, width),
        out_shape=(
            pltpu.VMEM((peers, own, value_dim), jnp.bfloat16),
            jax.ShapeDtypeStruct(cell.shape, jnp.float32),
            jax.ShapeDtypeStruct((own, key_dim), jnp.float32),
            jax.ShapeDtypeStruct((1, own), jnp.float32),
        ),
        in_specs=[vmem] * 3,
        out_specs=(vmem, hbm, hbm, hbm),
        scratch_shapes=[
            pltpu.VMEM(cell.shape, jnp.float32),
            pltpu.VMEM((own, key_dim), jnp.float32),
            pltpu.VMEM((1, own), jnp.float32),
            pltpu.SemaphoreType.DMA((own + 2,)),
        ],
        name="memory",
    )(*on_chip(tiles, cell, aux))


def on_device(
    tokens,
    gain_in,
    w_query,
    w_key,
    w_value,
    w_outgate,
    w_input_gate,
    w_forget_gate,
    bias_input,
    bias_forget,
    cell_state,
    norm_state,
    max_state,
    w_proj,
    gain_mid,
    w_up,
    w_down,
):
    seqs, own_columns = tokens.shape
    value_dim = cell_state.shape[3]
    tp, kv = lax.axis_size("tp"), lax.axis_size("kv")
    rows = gain_in.shape[0]
    width = rows * kv
    own = seqs // kv
    key_dim = cell_state.shape[2]
    heads_all = w_input_gate.shape[1]
    is_head = lax.broadcasted_iota(jnp.int32, (1, heads_all), 1) == lax.axis_index("tp")
    pick = is_head.astype(jnp.float32)
    aux_in = jnp.concatenate(
        [gain_in.reshape(1, rows), jnp.pad(pick, ((0, 0), (0, rows - heads_all)))], axis=0
    )
    biases = jnp.stack([jnp.sum(bias_input * pick[0]), jnp.sum(bias_forget * pick[0])])
    aux = jnp.concatenate(
        [norm_state[:, 0], max_state, jnp.broadcast_to(biases, (own, 2))], axis=1
    )
    aux = jnp.pad(aux, ((0, 0), (0, LANES - key_dim - 3)))

    own_tokens = tokens.T
    gathered, aux_in, aux, residual = lax.optimization_barrier(
        (spread(own_tokens, "tp"), aux_in, aux, own_tokens.astype(jnp.float32))
    )
    weights = (w_query.T, w_key.T, w_value, w_outgate, w_input_gate.T, w_forget_gate.T)
    terms = project(gathered, aux_in, weights, kv)
    heads, cell_new, norm_new, max_new = memory_step(
        exchange(terms, "kv"), cell_state[:, 0], aux, width
    )

    heads = exchange(heads, "kv").reshape(seqs, value_dim)
    branch = contract(w_proj, heads, 0, 1).astype(jnp.bfloat16)
    branch = exchange(branch.reshape(tp, own_columns, seqs), "tp")
    own_middle = residual + jnp.sum(branch.astype(jnp.float32), axis=0)
    own_middle = own_middle.astype(jnp.bfloat16)
    middle = spread(own_middle, "tp").reshape(rows, seqs).astype(jnp.float32)
    mid_squares = jnp.sum(middle * middle, axis=0)
    normed_mid = (middle * gain_mid[:, None]).astype(jnp.bfloat16)
    upward = contract(normed_mid, w_up, 0, 0)
    upward = jnp.concatenate([upward, mid_squares[:, None]], axis=1).astype(jnp.bfloat16)
    upward = exchange(upward.reshape(kv, own, -1), "kv")
    upward = jnp.sum(upward.astype(jnp.float32), axis=0)
    scale_mid = lax.rsqrt(upward[:, -1:] / width + EPSILON)
    hidden = jnp.square(jax.nn.relu(upward[:, :-1] * scale_mid)).astype(jnp.bfloat16)

    hidden = spread(hidden, "kv").reshape(seqs, -1)
    down = contract(w_down, hidden, 0, 1).astype(jnp.bfloat16)
    down = exchange(down.reshape(tp, own_columns, seqs), "tp")
    mixed = own_middle.astype(jnp.float32) + jnp.sum(down.astype(jnp.float32), axis=0)
    mixed = mixed.astype(jnp.bfloat16).T
    return (mixed, cell_new[:, None], norm_new[:, None], max_new.reshape(own, 1))


def solution(mesh):
    in_specs = (
        P("grp", ("kv", "tp")),
        P("kv"),
        P("kv", "tp"),
        P("kv", "tp"),
        P("kv", "tp"),
        P("kv", "tp"),
        P("kv", None),
        P("kv", None),
        P(),
        P(),
        P(("grp", "kv"), "tp", None, None),
        P(("grp", "kv"), "tp", None),
        P(("grp", "kv"), "tp"),
        P("tp", "kv"),
        P("kv"),
        P("kv", "tp"),
        P("tp", "kv"),
    )
    out_specs = (
        P("grp", ("kv", "tp")),
        P(("grp", "kv"), "tp", None, None),
        P(("grp", "kv"), "tp", None),
        P(("grp", "kv"), "tp"),
    )
    return jax.shard_map(
        on_device, mesh=mesh, in_specs=in_specs, out_specs=out_specs, check_vma=False
    )
```

```python
import functools

import jax
import jax.numpy as jnp
from jax import lax
from jax.experimental import pallas as pl
from jax.experimental.pallas import tpu as pltpu
from jax.sharding import PartitionSpec as P

EPSILON = 1e-06
LANES = 128


KV = ("kv_pair", "kv_side")


def exchange(tiles, axis):
    return lax.all_to_all(tiles, axis, split_axis=0, concat_axis=0, tiled=True)


def spread(value, axis):
    return exchange(jnp.broadcast_to(value, (lax.axis_size(axis), *value.shape)), axis)


def contract(left, right, left_dim, right_dim):
    dims = (((left_dim,), (right_dim,)), ((), ()))
    return lax.dot_general(left, right, dims, preferred_element_type=jnp.float32)


def two_parts(value):
    high = value.astype(jnp.bfloat16).astype(jnp.float32)
    return high, (value - high).astype(jnp.bfloat16).astype(jnp.float32)


def project_body(
    tokens, gain, pick, norm, top, bias_in, bias_forget,
    wq, wk, wv, wo, wi, wf, out, aux, residual,
):
    gain, pick = gain[...], pick[...]
    mine = jnp.zeros(residual.shape, jnp.float32)
    for peer in range(tokens.shape[0]):
        mine += tokens[peer].astype(jnp.float32) * pick[:, peer : peer + 1]
    residual[...] = mine
    count, key_dim = norm.shape
    place = lax.broadcasted_iota(jnp.int32, (count, LANES - key_dim), 1)
    first = jnp.sum(bias_in[...] * pick, axis=1, keepdims=True)
    second = jnp.sum(bias_forget[...] * pick, axis=1, keepdims=True)
    eye = lax.broadcasted_iota(jnp.int32, (count, count), 0)
    eye = eye == lax.broadcasted_iota(jnp.int32, (count, count), 1)
    turned = jnp.sum(jnp.where(eye, top[...], 0.0), axis=1, keepdims=True)
    rest = jnp.where(place == 1, first, jnp.where(place == 2, second, 0.0))
    rest = jnp.where(place == 0, turned, rest)
    aux[...] = jnp.concatenate([norm[...], rest], axis=1)
    wide = tokens[...].reshape(-1, tokens.shape[-1]).astype(jnp.float32).T
    squares = jnp.sum(wide * wide, axis=1, keepdims=True)
    normed = (wide * gain).astype(jnp.bfloat16)
    query = contract(normed, wq[...], 1, 1)
    keys = contract(normed, wk[...], 1, 1)
    values = contract(normed, wv[...], 1, 0)
    outgate = contract(normed, wo[...], 1, 0)
    gate_in = jnp.sum(contract(normed, wi[...], 1, 1) * pick, axis=1, keepdims=True)
    gate_forget = jnp.sum(contract(normed, wf[...], 1, 1) * pick, axis=1, keepdims=True)
    lane = lax.broadcasted_iota(jnp.int32, (wide.shape[0], LANES), 1)
    extra = jnp.zeros((wide.shape[0], LANES), jnp.float32)
    for place, value in enumerate((gate_in, gate_forget, squares)):
        high, low = two_parts(value)
        extra = jnp.where(lane == place, high, extra)
        extra = jnp.where(lane == place + 3, low, extra)
    both = jnp.concatenate([query, keys], axis=1)
    peers, own, _ = out.shape
    at = 0
    for piece in (both, values, outgate, extra):
        piece = piece.astype(jnp.bfloat16)
        for peer in range(peers):
            out[peer, :, at : at + LANES] = piece[peer * own : (peer + 1) * own]
        at += LANES


def memory_body(
    width, tiles, cell, aux,
    heads, cell_out, norm_out, top_out, cell_new, norm_buf, top_buf, sems,
):
    own, key_dim, value_dim = cell.shape
    terms = jnp.sum(tiles[...].astype(jnp.float32), axis=0)
    extra = terms[:, 3 * LANES :]
    extra = extra[:, 0:3] + extra[:, 3:6]
    scale = lax.rsqrt(extra[:, 2:3] / width + EPSILON)
    side = aux[...]
    norm, top = side[:, :key_dim], side[:, key_dim : key_dim + 1]
    log_input = extra[:, 0:1] * scale + side[:, key_dim + 1 : key_dim + 2]
    forget = extra[:, 1:2] * scale + side[:, key_dim + 2 : key_dim + 3]
    log_forget = jnp.minimum(forget, 0.0) - jnp.log1p(jnp.exp(-jnp.abs(forget)))
    log_keep = log_forget + top
    max_new = jnp.maximum(log_keep, log_input)
    keep = jnp.exp(log_keep - max_new)
    write = jnp.exp(log_input - max_new)
    top_buf[...] = jnp.broadcast_to(max_new, (own, LANES)).T[0:1]
    lane = lax.broadcasted_iota(jnp.int32, (own, LANES), 1)
    is_query = lane < key_dim
    both = terms[:, :LANES] * jnp.where(is_query, scale * key_dim ** (-0.5), scale * write)
    values = terms[:, LANES : 2 * LANES] * scale
    outgate = terms[:, 2 * LANES : 3 * LANES] * scale
    turned = jnp.concatenate([both] * (LANES // own), axis=0).T
    norm_new = keep * norm + both[:, key_dim:]
    norm_buf[...] = norm_new
    copies = [
        pltpu.make_async_copy(top_buf, top_out, sems.at[own]),
        pltpu.make_async_copy(norm_buf, norm_out, sems.at[own + 1]),
    ]
    for copy in copies:
        copy.start()
    rows = []
    for s in range(own):
        fresh = keep[s : s + 1] * cell[s] + turned[key_dim:, s : s + 1] * values[s : s + 1]
        cell_new[s] = fresh
        copies.append(pltpu.make_async_copy(cell_new.at[s], cell_out.at[s], sems.at[s]))
        copies[-1].start()
        rows.append(jnp.sum(turned[:key_dim, s : s + 1] * fresh, axis=0, keepdims=True))
    numer = jnp.concatenate(rows, axis=0)
    dot = jnp.sum(both[:, :key_dim] * norm_new, axis=1, keepdims=True)
    denom = jnp.maximum(jnp.abs(dot), jnp.exp(-max_new))
    done = (numer * (1.0 / (1.0 + jnp.exp(-outgate))) / denom).astype(jnp.bfloat16)
    for peer in range(heads.shape[0]):
        heads[peer] = done
    for copy in copies:
        copy.wait()


def on_chip(*arrays):
    return [pltpu.with_memory_space_constraint(a, pltpu.VMEM) for a in arrays]


def trade_body(w_up, w_down, gain, sent, gains, sems):
    other = 1 - lax.axis_index("kv_side")
    rows, columns = w_up.shape
    half = columns // 2
    at = pl.multiple_of(other * half, half)
    copies = [
        pltpu.make_async_copy(
            w_up.at[:, pl.ds(at, half)], sent.at[pl.ds(0, rows), pl.ds(0, half)], sems.at[0]
        )
    ]
    for part in range(half // rows):
        first = pl.multiple_of(at + part * rows, rows)
        copies.append(
            pltpu.make_async_copy(
                w_down.at[pl.ds(first, rows)],
                sent.at[pl.ds(0, rows), pl.ds(half + part * rows, rows)],
                sems.at[1 + part],
            )
        )
    for copy in copies:
        copy.start()
    high, low = two_parts(gain[...])
    line = lax.broadcasted_iota(jnp.int32, (gains.shape[0], rows), 0)
    both = jnp.where(line == 0, high, jnp.where(line == 1, low, 0.0))
    gains[...] = jnp.zeros(gains.shape, gains.dtype)
    gains[:, :rows] = both.astype(jnp.bfloat16)
    last = pltpu.make_async_copy(gains, sent.at[pl.ds(rows, gains.shape[0])], sems.at[3])
    last.start()
    for copy in (*copies, last):
        copy.wait()


def up_body(middle, gain, w_up, taken, out):
    side = lax.axis_index("kv_side")
    rows, columns = w_up.shape
    half = columns // 2
    count = middle.shape[0] // 2
    mine = middle[pl.ds(side * count, count)].reshape(rows, -1).astype(jnp.float32).T
    theirs = middle[pl.ds((1 - side) * count, count)].reshape(rows, -1).astype(jnp.float32).T
    squares = jnp.sum(mine * mine + theirs * theirs, axis=1, keepdims=True)
    gains = taken[rows : rows + 8, :rows].astype(jnp.float32)
    mine = (mine * gain[...]).astype(jnp.bfloat16)
    theirs = (theirs * (gains[0:1] + gains[1:2])).astype(jnp.bfloat16)
    upward = contract(mine, w_up[:, pl.ds(pl.multiple_of(side * half, half), half)], 1, 0)
    upward = upward + contract(theirs, taken[:rows, :half], 1, 0)
    lane = lax.broadcasted_iota(jnp.int32, (mine.shape[0], LANES), 1)
    high, low = two_parts(squares)
    extra = jnp.where(lane == 0, high, jnp.where(lane == 1, low, 0.0)).astype(jnp.bfloat16)
    upward = upward.astype(jnp.bfloat16)
    peers, own, _ = out.shape
    for peer in range(peers):
        out[peer, :, :half] = upward[peer * own : (peer + 1) * own]
        out[peer, :, half:] = extra[peer * own : (peer + 1) * own]


def down_body(hidden, w_down, taken, out):
    side = lax.axis_index("kv_side")
    rows = w_down.shape[1]
    half = hidden.shape[2]
    count = out.shape[0] // 2
    left = hidden[...].reshape(-1, half)
    mine = contract(left, w_down[pl.ds(pl.multiple_of(side * half, half), half)], 1, 0)
    theirs = contract(left[:, :rows], taken[:rows, half : half + rows], 1, 0)
    for part in range(1, half // rows):
        block = taken[:rows, half + part * rows : half + (part + 1) * rows]
        theirs = theirs + contract(left[:, part * rows : (part + 1) * rows], block, 1, 0)
    shape = (count, *out.shape[1:])
    out[pl.ds(side * count, count)] = mine.T.astype(jnp.bfloat16).reshape(shape)
    out[pl.ds((1 - side) * count, count)] = theirs.T.astype(jnp.bfloat16).reshape(shape)


def trade(w_up, w_down, gain):
    rows, columns = w_up.shape
    hbm = pl.BlockSpec(memory_space=pl.ANY)
    return pl.pallas_call(
        trade_body,
        out_shape=jax.ShapeDtypeStruct((rows + 8, columns), jnp.bfloat16),
        in_specs=[hbm, hbm, pl.BlockSpec(memory_space=pltpu.VMEM)],
        out_specs=hbm,
        scratch_shapes=[pltpu.VMEM((8, columns), jnp.bfloat16), pltpu.SemaphoreType.DMA((4,))],
        name="trade",
    )(w_up, w_down, gain)


def in_vmem(body, shape, *operands):
    vmem = pl.BlockSpec(memory_space=pltpu.VMEM)
    return pl.pallas_call(
        body,
        out_shape=pltpu.VMEM(shape, jnp.bfloat16),
        in_specs=[vmem] * len(operands),
        out_specs=vmem,
        name=body.__name__,
    )(*on_chip(*operands))


def project(tokens, small, weights, peers):
    seqs = tokens.shape[-1]
    own = seqs // peers
    vmem = pl.BlockSpec(memory_space=pltpu.VMEM)
    operands = on_chip(tokens, *small, *weights)
    return pl.pallas_call(
        project_body,
        out_shape=(
            pltpu.VMEM((peers, own, 4 * LANES), jnp.bfloat16),
            pltpu.VMEM((own, LANES), jnp.float32),
            pltpu.VMEM(tokens.shape[1:], jnp.float32),
        ),
        in_specs=[vmem] * len(operands),
        out_specs=(vmem,) * 3,
        name="project",
    )(*operands)


def memory_step(tiles, cell, aux, width):
    peers, own, _ = tiles.shape
    _, key_dim, value_dim = cell.shape
    vmem = pl.BlockSpec(memory_space=pltpu.VMEM)
    hbm = pl.BlockSpec(memory_space=pl.ANY)
    return pl.pallas_call(
        functools.partial(memory_body, width),
        out_shape=(
            pltpu.VMEM((peers, own, value_dim), jnp.bfloat16),
            jax.ShapeDtypeStruct(cell.shape, jnp.float32),
            jax.ShapeDtypeStruct((own, key_dim), jnp.float32),
            jax.ShapeDtypeStruct((1, own), jnp.float32),
        ),
        in_specs=[vmem] * 3,
        out_specs=(vmem, hbm, hbm, hbm),
        scratch_shapes=[
            pltpu.VMEM(cell.shape, jnp.float32),
            pltpu.VMEM((own, key_dim), jnp.float32),
            pltpu.VMEM((1, own), jnp.float32),
            pltpu.SemaphoreType.DMA((own + 2,)),
        ],
        name="memory",
    )(*on_chip(tiles, cell, aux))


def on_device(
    tokens,
    gain_in,
    w_query,
    w_key,
    w_value,
    w_outgate,
    w_input_gate,
    w_forget_gate,
    bias_input,
    bias_forget,
    cell_state,
    norm_state,
    max_state,
    w_proj,
    gain_mid,
    w_up,
    w_down,
):
    seqs, own_columns = tokens.shape
    value_dim = cell_state.shape[3]
    tp, kv = lax.axis_size("tp"), lax.axis_size(KV)
    pairs = kv // 2
    half = w_up.shape[1] // 2
    rows = gain_in.shape[0]
    width = rows * kv
    own = seqs // kv
    key_dim = cell_state.shape[2]
    heads_all = w_input_gate.shape[1]
    is_head = lax.broadcasted_iota(jnp.int32, (1, heads_all), 1) == lax.axis_index("tp")
    pick = is_head.astype(jnp.float32)

    copies = jnp.broadcast_to(tokens.T, (tp, own_columns, seqs))
    copies, pick = lax.optimization_barrier((copies, pick))
    small = (
        gain_in.reshape(1, rows),
        pick,
        norm_state[:, 0],
        max_state.reshape(1, own),
        bias_input.reshape(1, heads_all),
        bias_forget.reshape(1, heads_all),
    )
    weights = (w_query.T, w_key.T, w_value, w_outgate, w_input_gate.T, w_forget_gate.T)
    terms, aux, residual = project(exchange(copies, "tp"), small, weights, kv)
    heads, cell_new, norm_new, max_new = memory_step(
        exchange(terms, KV), cell_state[:, 0], aux, width
    )

    heads = exchange(heads, KV).reshape(seqs, value_dim)
    gain_mid = gain_mid.reshape(1, rows)
    gain_late, heads = lax.optimization_barrier((gain_mid, heads))
    taken = lax.ppermute(trade(w_up, w_down, gain_late), "kv_side", [(0, 1), (1, 0)])

    branch = contract(w_proj, heads, 0, 1).astype(jnp.bfloat16)
    branch = exchange(branch.reshape(tp, own_columns, seqs), "tp")
    own_middle = residual + jnp.sum(branch.astype(jnp.float32), axis=0)
    own_middle = own_middle.astype(jnp.bfloat16)
    middle = spread(own_middle, ("kv_side", "tp"))
    upward = in_vmem(up_body, (pairs, 2 * own, half + LANES), middle, gain_mid, w_up, taken)
    upward = jnp.sum(exchange(upward, "kv_pair").astype(jnp.float32), axis=0)
    total = upward[:, half : half + 1] + upward[:, half + 1 : half + 2]
    scale_mid = lax.rsqrt(total / width + EPSILON)
    hidden = jnp.square(jax.nn.relu(upward[:, :half] * scale_mid)).astype(jnp.bfloat16)

    hidden = spread(hidden, "kv_pair")
    down = in_vmem(down_body, (2 * tp, own_columns, seqs), hidden, w_down, taken)
    down = exchange(down, ("kv_side", "tp"))
    mixed = own_middle.astype(jnp.float32) + jnp.sum(down.astype(jnp.float32), axis=0)
    mixed = mixed.astype(jnp.bfloat16).T
    return (mixed, cell_new[:, None], norm_new[:, None], max_new.reshape(own, 1))


def solution(mesh):
    sizes = mesh.devices.shape
    halves = (sizes[0], sizes[1] // 2, 2, sizes[2])
    mesh = jax.sharding.Mesh(mesh.devices.reshape(halves), ("grp", *KV, "tp"))
    in_specs = (
        P("grp", (*KV, "tp")),
        P(KV),
        P(KV, "tp"),
        P(KV, "tp"),
        P(KV, "tp"),
        P(KV, "tp"),
        P(KV, None),
        P(KV, None),
        P(),
        P(),
        P(("grp", *KV), "tp", None, None),
        P(("grp", *KV), "tp", None),
        P(("grp", *KV), "tp"),
        P("tp", KV),
        P(KV),
        P(KV, "tp"),
        P("tp", KV),
    )
    out_specs = (
        P("grp", (*KV, "tp")),
        P(("grp", *KV), "tp", None, None),
        P(("grp", *KV), "tp", None),
        P(("grp", *KV), "tp"),
    )
    return jax.shard_map(
        on_device, mesh=mesh, in_specs=in_specs, out_specs=out_specs, check_vma=False
    )
```

```python
import functools

import jax
import jax.numpy as jnp
from jax import lax
from jax.experimental import pallas as pl
from jax.experimental.pallas import tpu as pltpu
from jax.sharding import PartitionSpec as P


EPSILON = 1e-06
LANES = 128


KV = ("kv_pair", "kv_side")


def exchange(tiles, axis):
    return lax.all_to_all(tiles, axis, split_axis=0, concat_axis=0, tiled=True)


def spread(value, axis):
    return exchange(jnp.broadcast_to(value, (lax.axis_size(axis), *value.shape)), axis)


def contract(left, right, left_dim, right_dim):
    dims = (((left_dim,), (right_dim,)), ((), ()))
    return lax.dot_general(left, right, dims, preferred_element_type=jnp.float32)


def two_parts(value):
    high = value.astype(jnp.bfloat16).astype(jnp.float32)
    return high, (value - high).astype(jnp.bfloat16).astype(jnp.float32)


def project_body(
    tokens, gain, pick, norm, top, bias_in, bias_forget,
    wq, wk, wv, wo, wi, wf, out, aux, residual,
):
    gain, pick = gain[...], pick[...]
    mine = jnp.zeros(residual.shape, jnp.float32)
    for peer in range(tokens.shape[0]):
        mine += tokens[peer].astype(jnp.float32) * pick[:, peer : peer + 1]
    residual[...] = mine
    count, key_dim = norm.shape
    place = lax.broadcasted_iota(jnp.int32, (count, LANES - key_dim), 1)
    first = jnp.sum(bias_in[...] * pick, axis=1, keepdims=True)
    second = jnp.sum(bias_forget[...] * pick, axis=1, keepdims=True)
    eye = lax.broadcasted_iota(jnp.int32, (count, count), 0)
    eye = eye == lax.broadcasted_iota(jnp.int32, (count, count), 1)
    turned = jnp.sum(jnp.where(eye, top[...], 0.0), axis=1, keepdims=True)
    rest = jnp.where(place == 1, first, jnp.where(place == 2, second, 0.0))
    rest = jnp.where(place == 0, turned, rest)
    aux[...] = jnp.concatenate([norm[...], rest], axis=1)
    wide = tokens[...].reshape(-1, tokens.shape[-1]).astype(jnp.float32).T
    squares = jnp.sum(wide * wide, axis=1, keepdims=True)
    normed = (wide * gain).astype(jnp.bfloat16)
    query = contract(normed, wq[...], 1, 1)
    keys = contract(normed, wk[...], 1, 1)
    values = contract(normed, wv[...], 1, 0)
    outgate = contract(normed, wo[...], 1, 0)
    gate_in = jnp.sum(contract(normed, wi[...], 1, 1) * pick, axis=1, keepdims=True)
    gate_forget = jnp.sum(contract(normed, wf[...], 1, 1) * pick, axis=1, keepdims=True)
    lane = lax.broadcasted_iota(jnp.int32, (wide.shape[0], LANES), 1)
    extra = jnp.zeros((wide.shape[0], LANES), jnp.float32)
    for place, value in enumerate((gate_in, gate_forget, squares)):
        high, low = two_parts(value)
        extra = jnp.where(lane == place, high, extra)
        extra = jnp.where(lane == place + 3, low, extra)
    both = jnp.concatenate([query, keys], axis=1)
    peers, own, _ = out.shape
    at = 0
    for piece in (both, values, outgate, extra):
        piece = piece.astype(jnp.bfloat16)
        for peer in range(peers):
            out[peer, :, at : at + LANES] = piece[peer * own : (peer + 1) * own]
        at += LANES


def memory_body(
    width, tiles, cell, aux, gain, w_up, w_down,
    heads, cell_out, norm_out, top_out, sent_up, sent_down, cell_new, norm_buf, top_buf, sems,
):
    rows, columns = w_up.shape
    half = columns // 2
    at = pl.multiple_of((1 - lax.axis_index("kv_side")) * half, half)
    last = sems.shape[0] - 1
    copies = [
        pltpu.make_async_copy(
            w_up.at[:, pl.ds(at, half)], sent_up.at[pl.ds(0, rows)], sems.at[last - 1]
        ),
        pltpu.make_async_copy(w_down.at[pl.ds(at, half)], sent_down, sems.at[last]),
    ]
    for copy in copies:
        copy.start()
    high, low = two_parts(gain[...])
    line = lax.broadcasted_iota(jnp.int32, (8, rows), 0)
    both = jnp.where(line == 0, high, jnp.where(line == 1, low, 0.0))
    sent_up[rows:, :rows] = both.astype(jnp.bfloat16)
    sent_up[rows:, rows:] = jnp.zeros((8, half - rows), jnp.bfloat16)
    own, key_dim, _ = cell.shape
    terms = jnp.sum(tiles[...].astype(jnp.float32), axis=0)
    extra = terms[:, 3 * LANES :]
    extra = extra[:, 0:3] + extra[:, 3:6]
    scale = lax.rsqrt(extra[:, 2:3] / width + EPSILON)
    side = aux[...]
    norm, top = side[:, :key_dim], side[:, key_dim : key_dim + 1]
    log_input = extra[:, 0:1] * scale + side[:, key_dim + 1 : key_dim + 2]
    forget = extra[:, 1:2] * scale + side[:, key_dim + 2 : key_dim + 3]
    log_forget = jnp.minimum(forget, 0.0) - jnp.log1p(jnp.exp(-jnp.abs(forget)))
    log_keep = log_forget + top
    max_new = jnp.maximum(log_keep, log_input)
    keep = jnp.exp(log_keep - max_new)
    write = jnp.exp(log_input - max_new)
    top_buf[...] = jnp.broadcast_to(max_new, (own, LANES)).T[0:1]
    lane = lax.broadcasted_iota(jnp.int32, (own, LANES), 1)
    is_query = lane < key_dim
    both = terms[:, :LANES] * jnp.where(is_query, scale * key_dim ** (-0.5), scale * write)
    values = terms[:, LANES : 2 * LANES] * scale
    outgate = terms[:, 2 * LANES : 3 * LANES] * scale
    turned = jnp.concatenate([both] * (LANES // own), axis=0).T
    norm_new = keep * norm + both[:, key_dim:]
    norm_buf[...] = norm_new
    for buf, target, sem in ((top_buf, top_out, own), (norm_buf, norm_out, own + 1)):
        copies.append(pltpu.make_async_copy(buf, target, sems.at[sem]))
        copies[-1].start()
    rows = []
    for s in range(own):
        fresh = keep[s : s + 1] * cell[s] + turned[key_dim:, s : s + 1] * values[s : s + 1]
        cell_new[s] = fresh
        copies.append(pltpu.make_async_copy(cell_new.at[s], cell_out.at[s], sems.at[s]))
        copies[-1].start()
        rows.append(jnp.sum(turned[:key_dim, s : s + 1] * fresh, axis=0, keepdims=True))
    numer = jnp.concatenate(rows, axis=0)
    dot = jnp.sum(both[:, :key_dim] * norm_new, axis=1, keepdims=True)
    denom = jnp.maximum(jnp.abs(dot), jnp.exp(-max_new))
    done = (numer * (1.0 / (1.0 + jnp.exp(-outgate))) / denom).astype(jnp.bfloat16)
    for peer in range(heads.shape[0]):
        heads[peer] = done
    for copy in copies:
        copy.wait()


def on_chip(*arrays):
    return [pltpu.with_memory_space_constraint(a, pltpu.VMEM) for a in arrays]


def up_body(middle, gain, w_up, taken, out):
    side = lax.axis_index("kv_side")
    rows, columns = w_up.shape
    half = columns // 2
    count = middle.shape[0] // 2
    mine = middle[pl.ds(side * count, count)].reshape(rows, -1).astype(jnp.float32).T
    theirs = middle[pl.ds((1 - side) * count, count)].reshape(rows, -1).astype(jnp.float32).T
    squares = jnp.sum(mine * mine + theirs * theirs, axis=1, keepdims=True)
    gains = taken[rows : rows + 8, :rows].astype(jnp.float32)
    mine = (mine * gain[...]).astype(jnp.bfloat16)
    theirs = (theirs * (gains[0:1] + gains[1:2])).astype(jnp.bfloat16)
    upward = contract(mine, w_up[:, pl.ds(pl.multiple_of(side * half, half), half)], 1, 0)
    upward = upward + contract(theirs, taken[:rows], 1, 0)
    lane = lax.broadcasted_iota(jnp.int32, (mine.shape[0], LANES), 1)
    high, low = two_parts(squares)
    extra = jnp.where(lane == 0, high, jnp.where(lane == 1, low, 0.0)).astype(jnp.bfloat16)
    upward = upward.astype(jnp.bfloat16)
    peers, own, _ = out.shape
    for peer in range(peers):
        out[peer, :, :half] = upward[peer * own : (peer + 1) * own]
        out[peer, :, half:] = extra[peer * own : (peer + 1) * own]


def down_body(hidden, w_down, taken, out):
    side = lax.axis_index("kv_side")
    half = hidden.shape[2]
    count = out.shape[0] // 2
    left = hidden[...].reshape(-1, half)
    mine = contract(left, w_down[pl.ds(pl.multiple_of(side * half, half), half)], 1, 0)
    theirs = contract(left, taken[...], 1, 0)
    shape = (count, *out.shape[1:])
    out[pl.ds(side * count, count)] = mine.T.astype(jnp.bfloat16).reshape(shape)
    out[pl.ds((1 - side) * count, count)] = theirs.T.astype(jnp.bfloat16).reshape(shape)


def in_vmem(body, shape, *operands):
    vmem = pl.BlockSpec(memory_space=pltpu.VMEM)
    return pl.pallas_call(
        body,
        out_shape=pltpu.VMEM(shape, jnp.bfloat16),
        in_specs=[vmem] * len(operands),
        out_specs=vmem,
    )(*on_chip(*operands))


def project(tokens, small, weights, peers):
    seqs = tokens.shape[-1]
    own = seqs // peers
    vmem = pl.BlockSpec(memory_space=pltpu.VMEM)
    operands = on_chip(tokens, *small, *weights)
    return pl.pallas_call(
        project_body,
        out_shape=(
            pltpu.VMEM((peers, own, 4 * LANES), jnp.bfloat16),
            pltpu.VMEM((own, LANES), jnp.float32),
            pltpu.VMEM(tokens.shape[1:], jnp.float32),
        ),
        in_specs=[vmem] * len(operands),
        out_specs=(vmem,) * 3,
        name="project",
    )(*operands)


def memory_step(tiles, cell, aux, gain, w_up, w_down, width):
    peers, own, _ = tiles.shape
    _, key_dim, value_dim = cell.shape
    rows, columns = w_up.shape
    vmem = pl.BlockSpec(memory_space=pltpu.VMEM)
    hbm = pl.BlockSpec(memory_space=pl.ANY)
    return pl.pallas_call(
        functools.partial(memory_body, width),
        out_shape=(
            pltpu.VMEM((peers, own, value_dim), jnp.bfloat16),
            jax.ShapeDtypeStruct(cell.shape, jnp.float32),
            jax.ShapeDtypeStruct((own, key_dim), jnp.float32),
            jax.ShapeDtypeStruct((1, own), jnp.float32),
            pltpu.VMEM((rows + 8, columns // 2), jnp.bfloat16),
            pltpu.VMEM((columns // 2, rows), jnp.bfloat16),
        ),
        in_specs=[vmem] * 4 + [hbm] * 2,
        out_specs=(vmem, hbm, hbm, hbm, vmem, vmem),
        scratch_shapes=[
            pltpu.VMEM(cell.shape, jnp.float32),
            pltpu.VMEM((own, key_dim), jnp.float32),
            pltpu.VMEM((1, own), jnp.float32),
            pltpu.SemaphoreType.DMA((own + 4,)),
        ],
        name="memory",
    )(*on_chip(tiles, cell, aux, gain), w_up, w_down)


def layer(
    tokens,
    gain_in,
    w_query,
    w_key,
    w_value,
    w_outgate,
    w_input_gate,
    w_forget_gate,
    bias_input,
    bias_forget,
    cell_state,
    norm_state,
    max_state,
    w_proj,
    gain_mid,
    w_up,
    w_down,
):
    seqs, own_columns = tokens.shape
    value_dim = cell_state.shape[3]
    tp, kv = lax.axis_size("tp"), lax.axis_size(KV)
    pairs = kv // 2
    half = w_up.shape[1] // 2
    rows = gain_in.shape[0]
    width = rows * kv
    own = seqs // kv
    heads_all = w_input_gate.shape[1]
    is_head = lax.broadcasted_iota(jnp.int32, (1, heads_all), 1) == lax.axis_index("tp")
    pick = is_head.astype(jnp.float32)

    gain_mid = gain_mid.reshape(1, rows)
    swap = [(0, 1), (1, 0)]

    copies = jnp.broadcast_to(tokens.T, (tp, own_columns, seqs))
    copies, pick = lax.optimization_barrier((copies, pick))
    gathered = exchange(copies, "tp")
    small = (
        gain_in.reshape(1, rows),
        pick,
        norm_state[:, 0],
        max_state.reshape(1, own),
        bias_input.reshape(1, heads_all),
        bias_forget.reshape(1, heads_all),
    )
    weights = (w_query.T, w_key.T, w_value, w_outgate, w_input_gate.T, w_forget_gate.T)
    terms, aux, residual = project(gathered, small, weights, kv)
    heads, cell_new, norm_new, max_new, sent_up, sent_down = memory_step(
        exchange(terms, KV), cell_state[:, 0], aux, gain_mid, w_up, w_down, width
    )

    heads = exchange(heads, KV).reshape(seqs, value_dim)
    heads, sent_up, sent_down = lax.optimization_barrier((heads, sent_up, sent_down))
    other_up = lax.ppermute(sent_up, "kv_side", swap)
    other_down = lax.ppermute(sent_down, "kv_side", swap)
    branch = contract(w_proj, heads, 0, 1).astype(jnp.bfloat16)
    branch = exchange(branch.reshape(tp, own_columns, seqs), "tp")
    own_middle = residual + jnp.sum(branch.astype(jnp.float32), axis=0)
    own_middle = own_middle.astype(jnp.bfloat16)
    middle = spread(own_middle, ("kv_side", "tp"))
    upward = in_vmem(up_body, (pairs, 2 * own, half + LANES), middle, gain_mid, w_up, other_up)
    upward = exchange(upward, "kv_pair")
    upward = jnp.sum(upward.astype(jnp.float32), axis=0)
    total = upward[:, half : half + 1] + upward[:, half + 1 : half + 2]
    scale_mid = lax.rsqrt(total / width + EPSILON)
    hidden = jnp.square(jax.nn.relu(upward[:, :half] * scale_mid)).astype(jnp.bfloat16)

    hidden, other_down = lax.optimization_barrier((hidden, other_down))
    hidden = spread(hidden, "kv_pair")
    down = in_vmem(down_body, (2 * tp, own_columns, seqs), hidden, w_down, other_down)
    down = exchange(down, ("kv_side", "tp"))
    mixed = own_middle.astype(jnp.float32) + jnp.sum(down.astype(jnp.float32), axis=0)
    mixed = mixed.astype(jnp.bfloat16).T
    return (mixed, cell_new[:, None], norm_new[:, None], max_new.reshape(own, 1))


def solution(mesh):
    sizes = mesh.devices.shape
    halves = (sizes[0], sizes[1] // 2, 2, sizes[2])
    mesh = jax.sharding.Mesh(mesh.devices.reshape(halves), ("grp", *KV, "tp"))
    in_specs = (
        P("grp", (*KV, "tp")),
        P(KV),
        P(KV, "tp"),
        P(KV, "tp"),
        P(KV, "tp"),
        P(KV, "tp"),
        P(KV, None),
        P(KV, None),
        P(),
        P(),
        P(("grp", *KV), "tp", None, None),
        P(("grp", *KV), "tp", None),
        P(("grp", *KV), "tp"),
        P("tp", KV),
        P(KV),
        P(KV, "tp"),
        P("tp", KV),
    )
    out_specs = (
        P("grp", (*KV, "tp")),
        P(("grp", *KV), "tp", None, None),
        P(("grp", *KV), "tp", None),
        P(("grp", *KV), "tp"),
    )
    return jax.shard_map(layer, mesh=mesh, in_specs=in_specs, out_specs=out_specs, check_vma=False)
```

```python
import functools

import jax
import jax.numpy as jnp
from jax import lax
from jax.experimental import pallas as pl
from jax.experimental.pallas import tpu as pltpu
from jax.sharding import PartitionSpec as P


EPSILON = 1e-06
LANES = 128


KV = ("kv_pair", "kv_side")


def exchange(tiles, axis):
    return lax.all_to_all(tiles, axis, split_axis=0, concat_axis=0, tiled=True)


def spread(value, axis):
    return exchange(jnp.broadcast_to(value, (lax.axis_size(axis), *value.shape)), axis)


def contract(left, right, left_dim, right_dim):
    dims = (((left_dim,), (right_dim,)), ((), ()))
    return lax.dot_general(left, right, dims, preferred_element_type=jnp.float32)


def two_parts(value):
    high = value.astype(jnp.bfloat16).astype(jnp.float32)
    return high, (value - high).astype(jnp.bfloat16).astype(jnp.float32)


def stage_body(
    width, tokens, gain_in, gain_mid, wi, wf, bias_in, bias_forget, norm, top, wq, wk,
    copies, gates, aux, residual, gains, first_gain, second_gain, both_qk,
    own, wi_buf, wf_buf, bias_in_buf, bias_forget_buf, norm_buf, top_buf, sems,
):
    moves = (
        (tokens, own), (gain_in, first_gain), (gain_mid, second_gain), (wi, wi_buf), (wf, wf_buf),
        (bias_in, bias_in_buf), (bias_forget, bias_forget_buf), (norm, norm_buf), (top, top_buf),
        (wq, both_qk.at[pl.ds(0, wq.shape[0])]), (wk, both_qk.at[pl.ds(wq.shape[0], wk.shape[0])]),
    )
    moves = [
        pltpu.make_async_copy(source, target, sems.at[at])
        for at, (source, target) in enumerate(moves)
    ]
    for move in moves:
        move.start()
    for move in moves:
        move.wait()
    head = lax.axis_index("tp")
    value = own[...]
    for peer in range(copies.shape[0]):
        copies[peer] = value
    residual[...] = value.astype(jnp.float32)
    heads, rows = wi_buf.shape
    count, key_dim = norm_buf.shape
    down = lax.broadcasted_iota(jnp.int32, (heads, rows), 0) == head
    line = lax.broadcasted_iota(jnp.int32, (8, rows), 0)
    picked = [
        jnp.sum(jnp.where(down, w[...].astype(jnp.float32), 0.0), axis=0, keepdims=True)
        for w in (wi_buf, wf_buf)
    ]
    both = jnp.where(line == 0, picked[0], jnp.where(line == 1, picked[1], 0.0))
    gates[...] = both.astype(jnp.bfloat16)
    high, low = two_parts(second_gain[...])
    both = jnp.where(line == 0, high, jnp.where(line == 1, low, 0.0))
    gains[...] = both.astype(jnp.bfloat16)
    along = lax.broadcasted_iota(jnp.int32, (1, heads), 1) == head
    place = lax.broadcasted_iota(jnp.int32, (count, width - key_dim), 1)
    first, second = [
        jnp.sum(jnp.where(along, b[...], 0.0), axis=1, keepdims=True)
        for b in (bias_in_buf, bias_forget_buf)
    ]
    eye = lax.broadcasted_iota(jnp.int32, (count, count), 0)
    eye = eye == lax.broadcasted_iota(jnp.int32, (count, count), 1)
    turned = jnp.sum(jnp.where(eye, top_buf[...], 0.0), axis=1, keepdims=True)
    rest = jnp.where(place == 1, first, jnp.where(place == 2, second, 0.0))
    rest = jnp.where(place == 0, turned, rest)
    aux[...] = jnp.concatenate([norm_buf[...], rest], axis=1)


def project_body(tokens, gain, gates, wqk, wv, wo, out):
    wide = tokens[...].reshape(-1, tokens.shape[-1]).astype(jnp.float32).T
    squares = jnp.sum(wide * wide, axis=1, keepdims=True)
    normed = (wide * gain[...]).astype(jnp.bfloat16)
    both = contract(normed, wqk[...], 1, 1)
    values = contract(normed, wv[...], 1, 0)
    outgate = contract(normed, wo[...], 1, 0)
    gate = contract(normed, gates[...], 1, 1)
    lane = lax.broadcasted_iota(jnp.int32, (wide.shape[0], LANES), 1)
    extra = jnp.zeros((wide.shape[0], LANES), jnp.float32)
    for place, value in enumerate((gate[:, 0:1], gate[:, 1:2], squares)):
        high, low = two_parts(value)
        extra = jnp.where(lane == place, high, extra)
        extra = jnp.where(lane == place + 3, low, extra)
    peers, own, _ = out.shape
    at = 0
    for piece in (both, values, outgate, extra):
        piece = piece.astype(jnp.bfloat16)
        for peer in range(peers):
            out[peer, :, at : at + LANES] = piece[peer * own : (peer + 1) * own]
        at += LANES


def memory_body(
    width, tiles, cell, aux, gains, w_up, w_down,
    heads, cell_out, norm_out, top_out, sent_up, sent_down, cell_new, norm_buf, top_buf, sems,
):
    rows, columns = w_up.shape
    half = columns // 2
    at = pl.multiple_of((1 - lax.axis_index("kv_side")) * half, half)
    last = sems.shape[0] - 1
    copies = [
        pltpu.make_async_copy(
            w_up.at[:, pl.ds(at, half)], sent_up.at[pl.ds(0, rows)], sems.at[last - 1]
        ),
        pltpu.make_async_copy(w_down.at[pl.ds(at, half)], sent_down, sems.at[last]),
    ]
    for copy in copies:
        copy.start()
    sent_up[rows:, :rows] = gains[...]
    sent_up[rows:, rows:] = jnp.zeros((8, half - rows), jnp.bfloat16)
    own, key_dim, _ = cell.shape
    terms = jnp.sum(tiles[...].astype(jnp.float32), axis=0)
    extra = terms[:, 3 * LANES :]
    extra = extra[:, 0:3] + extra[:, 3:6]
    scale = lax.rsqrt(extra[:, 2:3] / width + EPSILON)
    side = aux[...]
    norm, top = side[:, :key_dim], side[:, key_dim : key_dim + 1]
    log_input = extra[:, 0:1] * scale + side[:, key_dim + 1 : key_dim + 2]
    forget = extra[:, 1:2] * scale + side[:, key_dim + 2 : key_dim + 3]
    log_forget = jnp.minimum(forget, 0.0) - jnp.log1p(jnp.exp(-jnp.abs(forget)))
    log_keep = log_forget + top
    max_new = jnp.maximum(log_keep, log_input)
    keep = jnp.exp(log_keep - max_new)
    write = jnp.exp(log_input - max_new)
    top_buf[...] = jnp.broadcast_to(max_new, (own, LANES)).T[0:1]
    lane = lax.broadcasted_iota(jnp.int32, (own, LANES), 1)
    is_query = lane < key_dim
    both = terms[:, :LANES] * jnp.where(is_query, scale * key_dim ** (-0.5), scale * write)
    values = terms[:, LANES : 2 * LANES] * scale
    outgate = terms[:, 2 * LANES : 3 * LANES] * scale
    turned = jnp.concatenate([both] * (LANES // own), axis=0).T
    norm_new = keep * norm + both[:, key_dim:]
    norm_buf[...] = norm_new
    for buf, target, sem in ((top_buf, top_out, own), (norm_buf, norm_out, own + 1)):
        copies.append(pltpu.make_async_copy(buf, target, sems.at[sem]))
        copies[-1].start()
    rows = []
    for s in range(own):
        fresh = keep[s : s + 1] * cell[s] + turned[key_dim:, s : s + 1] * values[s : s + 1]
        cell_new[s] = fresh
        copies.append(pltpu.make_async_copy(cell_new.at[s], cell_out.at[s], sems.at[s]))
        copies[-1].start()
        rows.append(jnp.sum(turned[:key_dim, s : s + 1] * fresh, axis=0, keepdims=True))
    numer = jnp.concatenate(rows, axis=0)
    dot = jnp.sum(both[:, :key_dim] * norm_new, axis=1, keepdims=True)
    denom = jnp.maximum(jnp.abs(dot), jnp.exp(-max_new))
    done = (numer * (1.0 / (1.0 + jnp.exp(-outgate))) / denom).astype(jnp.bfloat16)
    for peer in range(heads.shape[0]):
        heads[peer] = done
    for copy in copies:
        copy.wait()


def on_chip(*arrays):
    return [pltpu.with_memory_space_constraint(a, pltpu.VMEM) for a in arrays]


def up_body(middle, gain, w_up, taken, out):
    side = lax.axis_index("kv_side")
    rows, columns = w_up.shape
    half = columns // 2
    count = middle.shape[0] // 2
    mine = middle[pl.ds(side * count, count)].reshape(rows, -1).astype(jnp.float32).T
    theirs = middle[pl.ds((1 - side) * count, count)].reshape(rows, -1).astype(jnp.float32).T
    squares = jnp.sum(mine * mine + theirs * theirs, axis=1, keepdims=True)
    gains = taken[rows : rows + 8, :rows].astype(jnp.float32)
    mine = (mine * gain[...]).astype(jnp.bfloat16)
    theirs = (theirs * (gains[0:1] + gains[1:2])).astype(jnp.bfloat16)
    upward = contract(mine, w_up[:, pl.ds(pl.multiple_of(side * half, half), half)], 1, 0)
    upward = upward + contract(theirs, taken[:rows], 1, 0)
    high, low = two_parts(squares)
    upward = upward.astype(jnp.bfloat16)
    peers, tiles, lines, lanes = out.shape
    across = half // lanes
    own = (tiles - 1) // across * lines
    lane = lax.broadcasted_iota(jnp.int32, (lines, lanes), 1)
    for peer in range(peers):
        extra = jnp.zeros((lines, lanes), jnp.float32)
        for part in range(own // lines):
            at = peer * own + part * lines
            for tile in range(across):
                out[peer, part * across + tile] = upward[
                    at : at + lines, tile * lanes : (tile + 1) * lanes
                ]
            extra = jnp.where(lane == 2 * part, high[at : at + lines], extra)
            extra = jnp.where(lane == 2 * part + 1, low[at : at + lines], extra)
        out[peer, tiles - 1] = extra.astype(jnp.bfloat16)


def hidden_body(width, tiles, copies):
    terms = jnp.sum(tiles[...].astype(jnp.float32), axis=0)
    count, lines, lanes = terms.shape
    peers, own, half = copies.shape
    across = half // lanes
    for part in range(own // lines):
        total = terms[count - 1, :, 2 * part : 2 * part + 1]
        total = total + terms[count - 1, :, 2 * part + 1 : 2 * part + 2]
        scale = lax.rsqrt(total / width + EPSILON)
        for tile in range(across):
            upward = jnp.maximum(terms[part * across + tile] * scale, 0.0)
            upward = (upward * upward).astype(jnp.bfloat16)
            for peer in range(peers):
                copies[
                    peer, part * lines : (part + 1) * lines, tile * lanes : (tile + 1) * lanes
                ] = upward


def down_body(hidden, w_down, taken, out):
    side = lax.axis_index("kv_side")
    half = hidden.shape[2]
    count = out.shape[0] // 2
    left = hidden[...].reshape(-1, half)
    mine = contract(left, w_down[pl.ds(pl.multiple_of(side * half, half), half)], 1, 0)
    theirs = contract(left, taken[...], 1, 0)
    shape = (count, *out.shape[1:])
    out[pl.ds(side * count, count)] = mine.T.astype(jnp.bfloat16).reshape(shape)
    out[pl.ds((1 - side) * count, count)] = theirs.T.astype(jnp.bfloat16).reshape(shape)


def in_vmem(body, shape, *operands):
    vmem = pl.BlockSpec(memory_space=pltpu.VMEM)
    return pl.pallas_call(
        body,
        out_shape=pltpu.VMEM(shape, jnp.bfloat16),
        in_specs=[vmem] * len(operands),
        out_specs=vmem,
    )(*on_chip(*operands))


def stage(operands, peers):
    tokens, gain = operands[0], operands[1]
    wi, norm = operands[3], operands[7]
    vmem = pl.BlockSpec(memory_space=pltpu.VMEM)
    out_shape = (
        pltpu.VMEM((peers, *tokens.shape), jnp.bfloat16),
        pltpu.VMEM((8, wi.shape[1]), jnp.bfloat16),
        pltpu.VMEM((norm.shape[0], LANES), jnp.float32),
        pltpu.VMEM(tokens.shape, jnp.float32),
        pltpu.VMEM((8, wi.shape[1]), jnp.bfloat16),
        pltpu.VMEM(gain.shape, jnp.float32),
        pltpu.VMEM(gain.shape, jnp.float32),
        pltpu.VMEM((operands[9].shape[0] + operands[10].shape[0], wi.shape[1]), jnp.bfloat16),
    )
    scratch = [pltpu.VMEM(a.shape, a.dtype) for a in (tokens, *operands[3:9])]
    return pl.pallas_call(
        functools.partial(stage_body, LANES),
        out_shape=out_shape,
        in_specs=[pl.BlockSpec(memory_space=pl.ANY)] * len(operands),
        out_specs=(vmem,) * len(out_shape),
        scratch_shapes=[*scratch, pltpu.SemaphoreType.DMA((len(operands),))],
        name="stage",
    )(*operands)


def memory_step(tiles, cell, aux, gains, w_up, w_down, width):
    peers, own, _ = tiles.shape
    _, key_dim, value_dim = cell.shape
    rows, columns = w_up.shape
    vmem = pl.BlockSpec(memory_space=pltpu.VMEM)
    hbm = pl.BlockSpec(memory_space=pl.ANY)
    return pl.pallas_call(
        functools.partial(memory_body, width),
        out_shape=(
            pltpu.VMEM((peers, own, value_dim), jnp.bfloat16),
            jax.ShapeDtypeStruct(cell.shape, jnp.float32),
            jax.ShapeDtypeStruct((own, key_dim), jnp.float32),
            jax.ShapeDtypeStruct((1, own), jnp.float32),
            pltpu.VMEM((rows + 8, columns // 2), jnp.bfloat16),
            pltpu.VMEM((columns // 2, rows), jnp.bfloat16),
        ),
        in_specs=[vmem] * 4 + [hbm] * 2,
        out_specs=(vmem, hbm, hbm, hbm, vmem, vmem),
        scratch_shapes=[
            pltpu.VMEM(cell.shape, jnp.float32),
            pltpu.VMEM((own, key_dim), jnp.float32),
            pltpu.VMEM((1, own), jnp.float32),
            pltpu.SemaphoreType.DMA((own + 4,)),
        ],
        name="memory",
    )(*on_chip(tiles, cell, aux, gains), w_up, w_down)


def layer(
    tokens,
    gain_in,
    w_query,
    w_key,
    w_value,
    w_outgate,
    w_input_gate,
    w_forget_gate,
    bias_input,
    bias_forget,
    cell_state,
    norm_state,
    max_state,
    w_proj,
    gain_mid,
    w_up,
    w_down,
):
    seqs, own_columns = tokens.shape
    value_dim = cell_state.shape[3]
    tp, kv = lax.axis_size("tp"), lax.axis_size(KV)
    pairs = kv // 2
    half = w_up.shape[1] // 2
    rows = gain_in.shape[0]
    width = rows * kv
    own = seqs // kv
    heads_all = w_input_gate.shape[1]
    swap = [(0, 1), (1, 0)]

    copies, gates, aux, residual, gains, gain_in, gain_mid, w_qk = stage(
        (
            tokens.T,
            gain_in.reshape(1, rows),
            gain_mid.reshape(1, rows),
            w_input_gate.T,
            w_forget_gate.T,
            bias_input.reshape(1, heads_all),
            bias_forget.reshape(1, heads_all),
            norm_state[:, 0],
            max_state.reshape(1, own),
            w_query.T,
            w_key.T,
        ),
        tp,
    )
    terms = in_vmem(
        project_body,
        (kv, own, 4 * LANES),
        exchange(copies, "tp"),
        gain_in,
        gates,
        w_qk,
        w_value,
        w_outgate,
    )
    heads, cell_new, norm_new, max_new, sent_up, sent_down = memory_step(
        exchange(terms, KV), cell_state[:, 0], aux, gains, w_up, w_down, width
    )

    heads = exchange(heads, KV).reshape(seqs, value_dim)
    heads, sent_up, sent_down = lax.optimization_barrier((heads, sent_up, sent_down))
    other_up = lax.ppermute(sent_up, "kv_side", swap)
    other_down = lax.ppermute(sent_down, "kv_side", swap)
    branch = contract(w_proj, heads, 0, 1).astype(jnp.bfloat16)
    branch = exchange(branch.reshape(tp, own_columns, seqs), "tp")
    own_middle = residual + jnp.sum(branch.astype(jnp.float32), axis=0)
    own_middle = own_middle.astype(jnp.bfloat16)
    middle = spread(own_middle, ("kv_side", "tp"))
    tiles = 2 * own * half // (8 * LANES) + 1
    upward = in_vmem(up_body, (pairs, tiles, 8, LANES), middle, gain_mid, w_up, other_up)
    upward = exchange(upward, "kv_pair")
    copies = in_vmem(functools.partial(hidden_body, width), (pairs, 2 * own, half), upward)
    copies, other_down = lax.optimization_barrier((copies, other_down))
    hidden = exchange(copies, "kv_pair")
    down = in_vmem(down_body, (2 * tp, own_columns, seqs), hidden, w_down, other_down)
    down = exchange(down, ("kv_side", "tp"))
    mixed = own_middle.astype(jnp.float32) + jnp.sum(down.astype(jnp.float32), axis=0)
    mixed = mixed.astype(jnp.bfloat16).T
    return (mixed, cell_new[:, None], norm_new[:, None], max_new.reshape(own, 1))


def solution(mesh):
    sizes = mesh.devices.shape
    halves = (sizes[0], sizes[1] // 2, 2, sizes[2])
    mesh = jax.sharding.Mesh(mesh.devices.reshape(halves), ("grp", *KV, "tp"))
    in_specs = (
        P("grp", (*KV, "tp")),
        P(KV),
        P(KV, "tp"),
        P(KV, "tp"),
        P(KV, "tp"),
        P(KV, "tp"),
        P(KV, None),
        P(KV, None),
        P(),
        P(),
        P(("grp", *KV), "tp", None, None),
        P(("grp", *KV), "tp", None),
        P(("grp", *KV), "tp"),
        P("tp", KV),
        P(KV),
        P(KV, "tp"),
        P("tp", KV),
    )
    out_specs = (
        P("grp", (*KV, "tp")),
        P(("grp", *KV), "tp", None, None),
        P(("grp", *KV), "tp", None),
        P(("grp", *KV), "tp"),
    )
    return jax.shard_map(layer, mesh=mesh, in_specs=in_specs, out_specs=out_specs, check_vma=False)
```

```python
import functools

import jax
import jax.numpy as jnp
from jax import lax
from jax.experimental import pallas as pl
from jax.experimental.pallas import tpu as pltpu
from jax.sharding import PartitionSpec as P


EPSILON = 1e-06
LANES = 128


KV = ("kv_pair", "kv_side")


def exchange(tiles, axis):
    return lax.all_to_all(tiles, axis, split_axis=0, concat_axis=0, tiled=True)


def spread(value, axis):
    return exchange(jnp.broadcast_to(value, (lax.axis_size(axis), *value.shape)), axis)


def contract(left, right, left_dim, right_dim):
    dims = (((left_dim,), (right_dim,)), ((), ()))
    return lax.dot_general(left, right, dims, preferred_element_type=jnp.float32)


def two_parts(value):
    high = value.astype(jnp.bfloat16).astype(jnp.float32)
    return high, (value - high).astype(jnp.bfloat16).astype(jnp.float32)


def stage_body(
    width, tokens, gain_in, gain_mid, wi, wf, bias_in, bias_forget, norm, top, wq, wk,
    copies, gates, aux, residual, gains, first_gain, second_gain, both_qk,
    own, wi_buf, wf_buf, bias_in_buf, bias_forget_buf, norm_buf, top_buf, sems,
):
    moves = (
        (tokens, own), (gain_in, first_gain), (gain_mid, second_gain), (wi, wi_buf), (wf, wf_buf),
        (bias_in, bias_in_buf), (bias_forget, bias_forget_buf), (norm, norm_buf), (top, top_buf),
        (wq, both_qk.at[pl.ds(0, wq.shape[0])]), (wk, both_qk.at[pl.ds(wq.shape[0], wk.shape[0])]),
    )
    moves = [
        pltpu.make_async_copy(source, target, sems.at[at])
        for at, (source, target) in enumerate(moves)
    ]
    for move in moves:
        move.start()
    for move in moves:
        move.wait()
    head = lax.axis_index("tp")
    value = own[...]
    for peer in range(copies.shape[0]):
        copies[peer] = value
    residual[...] = value.astype(jnp.float32)
    heads, rows = wi_buf.shape
    count, key_dim = norm_buf.shape
    down = lax.broadcasted_iota(jnp.int32, (heads, rows), 0) == head
    line = lax.broadcasted_iota(jnp.int32, (8, rows), 0)
    picked = [
        jnp.sum(jnp.where(down, w[...].astype(jnp.float32), 0.0), axis=0, keepdims=True)
        for w in (wi_buf, wf_buf)
    ]
    both = jnp.where(line == 0, picked[0], jnp.where(line == 1, picked[1], 0.0))
    gates[...] = both.astype(jnp.bfloat16)
    high, low = two_parts(second_gain[...])
    both = jnp.where(line == 0, high, jnp.where(line == 1, low, 0.0))
    gains[...] = both.astype(jnp.bfloat16)
    along = lax.broadcasted_iota(jnp.int32, (1, heads), 1) == head
    place = lax.broadcasted_iota(jnp.int32, (count, width - key_dim), 1)
    first, second = [
        jnp.sum(jnp.where(along, b[...], 0.0), axis=1, keepdims=True)
        for b in (bias_in_buf, bias_forget_buf)
    ]
    eye = lax.broadcasted_iota(jnp.int32, (count, count), 0)
    eye = eye == lax.broadcasted_iota(jnp.int32, (count, count), 1)
    turned = jnp.sum(jnp.where(eye, top_buf[...], 0.0), axis=1, keepdims=True)
    rest = jnp.where(place == 1, first, jnp.where(place == 2, second, 0.0))
    rest = jnp.where(place == 0, turned, rest)
    aux[...] = jnp.concatenate([norm_buf[...], rest], axis=1)


def project_body(tokens, gain, gates, wqk, wv, wo, out):
    wide = tokens[...].reshape(-1, tokens.shape[-1]).astype(jnp.float32).T
    squares = jnp.sum(wide * wide, axis=1, keepdims=True)
    normed = (wide * gain[...]).astype(jnp.bfloat16)
    both = contract(normed, wqk[...], 1, 1)
    values = contract(normed, wv[...], 1, 0)
    outgate = contract(normed, wo[...], 1, 0)
    gate = contract(normed, gates[...], 1, 1)
    lane = lax.broadcasted_iota(jnp.int32, (wide.shape[0], LANES), 1)
    extra = jnp.zeros((wide.shape[0], LANES), jnp.float32)
    for place, value in enumerate((gate[:, 0:1], gate[:, 1:2], squares)):
        high, low = two_parts(value)
        extra = jnp.where(lane == place, high, extra)
        extra = jnp.where(lane == place + 3, low, extra)
    peers, own, _ = out.shape
    at = 0
    for piece in (both, values, outgate, extra):
        piece = piece.astype(jnp.bfloat16)
        for peer in range(peers):
            out[peer, :, at : at + LANES] = piece[peer * own : (peer + 1) * own]
        at += LANES


def memory_body(
    width, tiles, cell, aux, gains, w_up, w_down,
    heads, cell_out, norm_out, top_out, sent_up, sent_down, cell_new, norm_buf, top_buf, sems,
):
    rows, columns = w_up.shape
    half = columns // 2
    at = pl.multiple_of((1 - lax.axis_index("kv_side")) * half, half)
    last = sems.shape[0] - 1
    copies = [
        pltpu.make_async_copy(
            w_up.at[:, pl.ds(at, half)], sent_up.at[pl.ds(0, rows)], sems.at[last - 1]
        ),
        pltpu.make_async_copy(w_down.at[pl.ds(at, half)], sent_down, sems.at[last]),
    ]
    for copy in copies:
        copy.start()
    sent_up[rows:, :rows] = gains[...]
    sent_up[rows:, rows:] = jnp.zeros((8, half - rows), jnp.bfloat16)
    own, key_dim, _ = cell.shape
    terms = jnp.sum(tiles[...].astype(jnp.float32), axis=0)
    extra = terms[:, 3 * LANES :]
    extra = extra[:, 0:3] + extra[:, 3:6]
    scale = lax.rsqrt(extra[:, 2:3] / width + EPSILON)
    side = aux[...]
    norm, top = side[:, :key_dim], side[:, key_dim : key_dim + 1]
    log_input = extra[:, 0:1] * scale + side[:, key_dim + 1 : key_dim + 2]
    forget = extra[:, 1:2] * scale + side[:, key_dim + 2 : key_dim + 3]
    log_forget = jnp.minimum(forget, 0.0) - jnp.log1p(jnp.exp(-jnp.abs(forget)))
    log_keep = log_forget + top
    max_new = jnp.maximum(log_keep, log_input)
    keep = jnp.exp(log_keep - max_new)
    write = jnp.exp(log_input - max_new)
    top_buf[...] = jnp.broadcast_to(max_new, (own, LANES)).T[0:1]
    lane = lax.broadcasted_iota(jnp.int32, (own, LANES), 1)
    is_query = lane < key_dim
    both = terms[:, :LANES] * jnp.where(is_query, scale * key_dim ** (-0.5), scale * write)
    values = terms[:, LANES : 2 * LANES] * scale
    outgate = terms[:, 2 * LANES : 3 * LANES] * scale
    turned = jnp.concatenate([both] * (LANES // own), axis=0).T
    norm_new = keep * norm + both[:, key_dim:]
    norm_buf[...] = norm_new
    for buf, target, sem in ((top_buf, top_out, own), (norm_buf, norm_out, own + 1)):
        copies.append(pltpu.make_async_copy(buf, target, sems.at[sem]))
        copies[-1].start()
    rows = []
    for s in range(own):
        fresh = keep[s : s + 1] * cell[s] + turned[key_dim:, s : s + 1] * values[s : s + 1]
        cell_new[s] = fresh
        copies.append(pltpu.make_async_copy(cell_new.at[s], cell_out.at[s], sems.at[s]))
        copies[-1].start()
        rows.append(jnp.sum(turned[:key_dim, s : s + 1] * fresh, axis=0, keepdims=True))
    numer = jnp.concatenate(rows, axis=0)
    dot = jnp.sum(both[:, :key_dim] * norm_new, axis=1, keepdims=True)
    denom = jnp.maximum(jnp.abs(dot), jnp.exp(-max_new))
    done = (numer * (1.0 / (1.0 + jnp.exp(-outgate))) / denom).astype(jnp.bfloat16)
    for peer in range(heads.shape[0]):
        heads[peer] = done
    for copy in copies:
        copy.wait()


def on_chip(*arrays):
    return [pltpu.with_memory_space_constraint(a, pltpu.VMEM) for a in arrays]


def up_body(middle, gain, w_up, taken, out):
    side = lax.axis_index("kv_side")
    rows, columns = w_up.shape
    half = columns // 2
    count = middle.shape[0] // 2
    mine = middle[pl.ds(side * count, count)].reshape(rows, -1).astype(jnp.float32).T
    theirs = middle[pl.ds((1 - side) * count, count)].reshape(rows, -1).astype(jnp.float32).T
    squares = jnp.sum(mine * mine + theirs * theirs, axis=1, keepdims=True)
    gains = taken[rows : rows + 8, :rows].astype(jnp.float32)
    mine = (mine * gain[...]).astype(jnp.bfloat16)
    theirs = (theirs * (gains[0:1] + gains[1:2])).astype(jnp.bfloat16)
    upward = contract(mine, w_up[:, pl.ds(pl.multiple_of(side * half, half), half)], 1, 0)
    upward = upward + contract(theirs, taken[:rows], 1, 0)
    high, low = two_parts(squares)
    upward = upward.astype(jnp.bfloat16)
    peers, tiles, lines, lanes = out.shape
    across = half // lanes
    own = (tiles - 1) // across * lines
    lane = lax.broadcasted_iota(jnp.int32, (lines, lanes), 1)
    for peer in range(peers):
        extra = jnp.zeros((lines, lanes), jnp.float32)
        for part in range(own // lines):
            at = peer * own + part * lines
            for tile in range(across):
                out[peer, part * across + tile] = upward[
                    at : at + lines, tile * lanes : (tile + 1) * lanes
                ]
            extra = jnp.where(lane == 2 * part, high[at : at + lines], extra)
            extra = jnp.where(lane == 2 * part + 1, low[at : at + lines], extra)
        out[peer, tiles - 1] = extra.astype(jnp.bfloat16)


def hidden_body(width, tiles, out):
    terms = jnp.sum(tiles[...].astype(jnp.float32), axis=0)
    count, lines, lanes = terms.shape
    own, half = out.shape
    across = half // lanes
    for part in range(own // lines):
        total = terms[count - 1, :, 2 * part : 2 * part + 1]
        total = total + terms[count - 1, :, 2 * part + 1 : 2 * part + 2]
        scale = lax.rsqrt(total / width + EPSILON)
        for tile in range(across):
            upward = jnp.maximum(terms[part * across + tile] * scale, 0.0)
            out[part * lines : (part + 1) * lines, tile * lanes : (tile + 1) * lanes] = (
                upward * upward
            ).astype(jnp.bfloat16)


def down_body(hidden, w_down, taken, out):
    side = lax.axis_index("kv_side")
    half = hidden.shape[1]
    count = out.shape[0] // 2
    left = hidden[...]
    mine = contract(left, w_down[pl.ds(pl.multiple_of(side * half, half), half)], 1, 0)
    theirs = contract(left, taken[...], 1, 0)
    shape = (count, *out.shape[1:])
    out[pl.ds(side * count, count)] = mine.T.astype(jnp.bfloat16).reshape(shape)
    out[pl.ds((1 - side) * count, count)] = theirs.T.astype(jnp.bfloat16).reshape(shape)


def in_vmem(body, shape, *operands):
    vmem = pl.BlockSpec(memory_space=pltpu.VMEM)
    return pl.pallas_call(
        body,
        out_shape=pltpu.VMEM(shape, jnp.bfloat16),
        in_specs=[vmem] * len(operands),
        out_specs=vmem,
    )(*on_chip(*operands))


def stage(operands, peers):
    tokens, gain = operands[0], operands[1]
    wi, norm = operands[3], operands[7]
    vmem = pl.BlockSpec(memory_space=pltpu.VMEM)
    out_shape = (
        pltpu.VMEM((peers, *tokens.shape), jnp.bfloat16),
        pltpu.VMEM((8, wi.shape[1]), jnp.bfloat16),
        pltpu.VMEM((norm.shape[0], LANES), jnp.float32),
        pltpu.VMEM(tokens.shape, jnp.float32),
        pltpu.VMEM((8, wi.shape[1]), jnp.bfloat16),
        pltpu.VMEM(gain.shape, jnp.float32),
        pltpu.VMEM(gain.shape, jnp.float32),
        pltpu.VMEM((operands[9].shape[0] + operands[10].shape[0], wi.shape[1]), jnp.bfloat16),
    )
    scratch = [pltpu.VMEM(a.shape, a.dtype) for a in (tokens, *operands[3:9])]
    return pl.pallas_call(
        functools.partial(stage_body, LANES),
        out_shape=out_shape,
        in_specs=[pl.BlockSpec(memory_space=pl.ANY)] * len(operands),
        out_specs=(vmem,) * len(out_shape),
        scratch_shapes=[*scratch, pltpu.SemaphoreType.DMA((len(operands),))],
        name="stage",
    )(*operands)


def memory_step(tiles, cell, aux, gains, w_up, w_down, width):
    peers, own, _ = tiles.shape
    _, key_dim, value_dim = cell.shape
    rows, columns = w_up.shape
    vmem = pl.BlockSpec(memory_space=pltpu.VMEM)
    hbm = pl.BlockSpec(memory_space=pl.ANY)
    return pl.pallas_call(
        functools.partial(memory_body, width),
        out_shape=(
            pltpu.VMEM((peers, own, value_dim), jnp.bfloat16),
            jax.ShapeDtypeStruct(cell.shape, jnp.float32),
            jax.ShapeDtypeStruct((own, key_dim), jnp.float32),
            jax.ShapeDtypeStruct((1, own), jnp.float32),
            pltpu.VMEM((rows + 8, columns // 2), jnp.bfloat16),
            pltpu.VMEM((columns // 2, rows), jnp.bfloat16),
        ),
        in_specs=[vmem] * 4 + [hbm] * 2,
        out_specs=(vmem, hbm, hbm, hbm, vmem, vmem),
        scratch_shapes=[
            pltpu.VMEM(cell.shape, jnp.float32),
            pltpu.VMEM((own, key_dim), jnp.float32),
            pltpu.VMEM((1, own), jnp.float32),
            pltpu.SemaphoreType.DMA((own + 4,)),
        ],
        name="memory",
    )(*on_chip(tiles, cell, aux, gains), w_up, w_down)


def layer(
    tokens,
    gain_in,
    w_query,
    w_key,
    w_value,
    w_outgate,
    w_input_gate,
    w_forget_gate,
    bias_input,
    bias_forget,
    cell_state,
    norm_state,
    max_state,
    w_proj,
    gain_mid,
    w_up,
    w_down,
):
    seqs, own_columns = tokens.shape
    value_dim = cell_state.shape[3]
    tp, kv = lax.axis_size("tp"), lax.axis_size(KV)
    pairs = kv // 2
    half = w_up.shape[1] // 2
    rows = gain_in.shape[0]
    width = rows * kv
    own = seqs // kv
    heads_all = w_input_gate.shape[1]
    swap = [(0, 1), (1, 0)]

    copies, gates, aux, residual, gains, gain_in, gain_mid, w_qk = stage(
        (
            tokens.T,
            gain_in.reshape(1, rows),
            gain_mid.reshape(1, rows),
            w_input_gate.T,
            w_forget_gate.T,
            bias_input.reshape(1, heads_all),
            bias_forget.reshape(1, heads_all),
            norm_state[:, 0],
            max_state.reshape(1, own),
            w_query.T,
            w_key.T,
        ),
        tp,
    )
    terms = in_vmem(
        project_body,
        (kv, own, 4 * LANES),
        exchange(copies, "tp"),
        gain_in,
        gates,
        w_qk,
        w_value,
        w_outgate,
    )
    heads, cell_new, norm_new, max_new, sent_up, sent_down = memory_step(
        exchange(terms, KV), cell_state[:, 0], aux, gains, w_up, w_down, width
    )

    heads = exchange(heads, KV).reshape(seqs, value_dim)
    heads, sent_up, sent_down = lax.optimization_barrier((heads, sent_up, sent_down))
    other_up = lax.ppermute(sent_up, "kv_side", swap)
    other_down = lax.ppermute(sent_down, "kv_side", swap)
    branch = contract(w_proj, heads, 0, 1).astype(jnp.bfloat16)
    branch = exchange(branch.reshape(tp, own_columns, seqs), "tp")
    own_middle = residual + jnp.sum(branch.astype(jnp.float32), axis=0)
    own_middle = own_middle.astype(jnp.bfloat16)
    middle = spread(own_middle, ("kv_side", "tp"))
    tiles = 2 * own * half // (8 * LANES) + 1
    upward = in_vmem(up_body, (pairs, tiles, 8, LANES), middle, gain_mid, w_up, other_up)
    upward = exchange(upward, "kv_pair")
    hidden = in_vmem(functools.partial(hidden_body, width), (2 * own, half), upward)
    hidden, other_down = lax.optimization_barrier((hidden, other_down))
    hidden = lax.all_gather(hidden, "kv_pair", axis=0, tiled=True)
    down = in_vmem(down_body, (2 * tp, own_columns, seqs), hidden, w_down, other_down)
    down = exchange(down, ("kv_side", "tp"))
    mixed = own_middle.astype(jnp.float32) + jnp.sum(down.astype(jnp.float32), axis=0)
    mixed = mixed.astype(jnp.bfloat16).T
    return (mixed, cell_new[:, None], norm_new[:, None], max_new.reshape(own, 1))


def solution(mesh):
    sizes = mesh.devices.shape
    halves = (sizes[0], sizes[1] // 2, 2, sizes[2])
    mesh = jax.sharding.Mesh(mesh.devices.reshape(halves), ("grp", *KV, "tp"))
    in_specs = (
        P("grp", (*KV, "tp")),
        P(KV),
        P(KV, "tp"),
        P(KV, "tp"),
        P(KV, "tp"),
        P(KV, "tp"),
        P(KV, None),
        P(KV, None),
        P(),
        P(),
        P(("grp", *KV), "tp", None, None),
        P(("grp", *KV), "tp", None),
        P(("grp", *KV), "tp"),
        P("tp", KV),
        P(KV),
        P(KV, "tp"),
        P("tp", KV),
    )
    out_specs = (
        P("grp", (*KV, "tp")),
        P(("grp", *KV), "tp", None, None),
        P(("grp", *KV), "tp", None),
        P(("grp", *KV), "tp"),
    )
    return jax.shard_map(layer, mesh=mesh, in_specs=in_specs, out_specs=out_specs, check_vma=False)
```

```python
import functools

import jax
import jax.numpy as jnp
from jax import lax
from jax.experimental import pallas as pl
from jax.experimental.pallas import tpu as pltpu
from jax.sharding import PartitionSpec as P


EPSILON = 1e-06
LANES = 128


KV = ("kv_pair", "kv_side")


def exchange(tiles, axis):
    return lax.all_to_all(tiles, axis, split_axis=0, concat_axis=0, tiled=True)


def spread(value, axis):
    return exchange(jnp.broadcast_to(value, (lax.axis_size(axis), *value.shape)), axis)


def contract(left, right, left_dim, right_dim):
    dims = (((left_dim,), (right_dim,)), ((), ()))
    return lax.dot_general(left, right, dims, preferred_element_type=jnp.float32)


def two_parts(value):
    high = value.astype(jnp.bfloat16).astype(jnp.float32)
    return high, (value - high).astype(jnp.bfloat16).astype(jnp.float32)


def stage_body(
    width, tokens, gain_in, gain_mid, wi, wf, bias_in, bias_forget, norm, top, wq, wk,
    copies, gates, aux, residual, gains, first_gain, second_gain, both_qk,
    own, wi_buf, wf_buf, bias_in_buf, bias_forget_buf, norm_buf, top_buf, sems,
):
    moves = (
        (tokens, own), (gain_in, first_gain), (gain_mid, second_gain), (wi, wi_buf), (wf, wf_buf),
        (bias_in, bias_in_buf), (bias_forget, bias_forget_buf), (norm, norm_buf), (top, top_buf),
        (wq, both_qk.at[pl.ds(0, wq.shape[0])]), (wk, both_qk.at[pl.ds(wq.shape[0], wk.shape[0])]),
    )
    moves = [
        pltpu.make_async_copy(source, target, sems.at[at])
        for at, (source, target) in enumerate(moves)
    ]
    for move in moves:
        move.start()
    for move in moves:
        move.wait()
    head = lax.axis_index("tp")
    value = own[...]
    for peer in range(copies.shape[0]):
        copies[peer] = value
    residual[...] = value.astype(jnp.float32)
    heads, rows = wi_buf.shape
    count, key_dim = norm_buf.shape
    down = lax.broadcasted_iota(jnp.int32, (heads, rows), 0) == head
    line = lax.broadcasted_iota(jnp.int32, (8, rows), 0)
    picked = [
        jnp.sum(jnp.where(down, w[...].astype(jnp.float32), 0.0), axis=0, keepdims=True)
        for w in (wi_buf, wf_buf)
    ]
    both = jnp.where(line == 0, picked[0], jnp.where(line == 1, picked[1], 0.0))
    gates[...] = both.astype(jnp.bfloat16)
    high, low = two_parts(second_gain[...])
    both = jnp.where(line == 0, high, jnp.where(line == 1, low, 0.0))
    gains[...] = both.astype(jnp.bfloat16)
    along = lax.broadcasted_iota(jnp.int32, (1, heads), 1) == head
    place = lax.broadcasted_iota(jnp.int32, (count, width - key_dim), 1)
    first, second = [
        jnp.sum(jnp.where(along, b[...], 0.0), axis=1, keepdims=True)
        for b in (bias_in_buf, bias_forget_buf)
    ]
    eye = lax.broadcasted_iota(jnp.int32, (count, count), 0)
    eye = eye == lax.broadcasted_iota(jnp.int32, (count, count), 1)
    turned = jnp.sum(jnp.where(eye, top_buf[...], 0.0), axis=1, keepdims=True)
    rest = jnp.where(place == 1, first, jnp.where(place == 2, second, 0.0))
    rest = jnp.where(place == 0, turned, rest)
    aux[...] = jnp.concatenate([norm_buf[...], rest], axis=1)


def project_body(tokens, gain, gates, wqk, wv, wo, out):
    wide = tokens[...].reshape(-1, tokens.shape[-1]).astype(jnp.float32).T
    squares = jnp.sum(wide * wide, axis=1, keepdims=True)
    normed = (wide * gain[...]).astype(jnp.bfloat16)
    both = contract(normed, wqk[...], 1, 1)
    values = contract(normed, wv[...], 1, 0)
    outgate = contract(normed, wo[...], 1, 0)
    gate = contract(normed, gates[...], 1, 1)
    lane = lax.broadcasted_iota(jnp.int32, (wide.shape[0], LANES), 1)
    extra = jnp.zeros((wide.shape[0], LANES), jnp.float32)
    for place, value in enumerate((gate[:, 0:1], gate[:, 1:2], squares)):
        high, low = two_parts(value)
        extra = jnp.where(lane == place, high, extra)
        extra = jnp.where(lane == place + 3, low, extra)
    peers, own, _ = out.shape
    at = 0
    for piece in (both, values, outgate, extra):
        piece = piece.astype(jnp.bfloat16)
        for peer in range(peers):
            out[peer, :, at : at + LANES] = piece[peer * own : (peer + 1) * own]
        at += LANES


def memory_body(
    width, tiles, cell, aux, gains, w_up, w_down,
    heads, cell_out, norm_out, top_out, sent_up, sent_down, cell_new, norm_buf, top_buf, sems,
):
    rows, columns = w_up.shape
    half = columns // 2
    at = pl.multiple_of((1 - lax.axis_index("kv_side")) * half, half)
    last = sems.shape[0] - 1
    copies = [
        pltpu.make_async_copy(
            w_up.at[:, pl.ds(at, half)], sent_up.at[pl.ds(0, rows)], sems.at[last - 1]
        ),
        pltpu.make_async_copy(w_down.at[pl.ds(at, half)], sent_down, sems.at[last]),
    ]
    for copy in copies:
        copy.start()
    sent_up[rows:, :rows] = gains[...]
    sent_up[rows:, rows:] = jnp.zeros((8, half - rows), jnp.bfloat16)
    own, key_dim, _ = cell.shape
    terms = jnp.sum(tiles[...].astype(jnp.float32), axis=0)
    extra = terms[:, 3 * LANES :]
    extra = extra[:, 0:3] + extra[:, 3:6]
    scale = lax.rsqrt(extra[:, 2:3] / width + EPSILON)
    side = aux[...]
    norm, top = side[:, :key_dim], side[:, key_dim : key_dim + 1]
    log_input = extra[:, 0:1] * scale + side[:, key_dim + 1 : key_dim + 2]
    forget = extra[:, 1:2] * scale + side[:, key_dim + 2 : key_dim + 3]
    log_forget = jnp.minimum(forget, 0.0) - jnp.log1p(jnp.exp(-jnp.abs(forget)))
    log_keep = log_forget + top
    max_new = jnp.maximum(log_keep, log_input)
    keep = jnp.exp(log_keep - max_new)
    write = jnp.exp(log_input - max_new)
    top_buf[...] = jnp.broadcast_to(max_new, (own, LANES)).T[0:1]
    lane = lax.broadcasted_iota(jnp.int32, (own, LANES), 1)
    is_query = lane < key_dim
    both = terms[:, :LANES] * jnp.where(is_query, scale * key_dim ** (-0.5), scale * write)
    values = terms[:, LANES : 2 * LANES] * scale
    outgate = terms[:, 2 * LANES : 3 * LANES] * scale
    turned = jnp.concatenate([both] * (LANES // own), axis=0).T
    norm_new = keep * norm + both[:, key_dim:]
    norm_buf[...] = norm_new
    for buf, target, sem in ((top_buf, top_out, own), (norm_buf, norm_out, own + 1)):
        copies.append(pltpu.make_async_copy(buf, target, sems.at[sem]))
        copies[-1].start()
    rows = []
    for s in range(own):
        fresh = keep[s : s + 1] * cell[s] + turned[key_dim:, s : s + 1] * values[s : s + 1]
        cell_new[s] = fresh
        copies.append(pltpu.make_async_copy(cell_new.at[s], cell_out.at[s], sems.at[s]))
        copies[-1].start()
        rows.append(jnp.sum(turned[:key_dim, s : s + 1] * fresh, axis=0, keepdims=True))
    numer = jnp.concatenate(rows, axis=0)
    dot = jnp.sum(both[:, :key_dim] * norm_new, axis=1, keepdims=True)
    denom = jnp.maximum(jnp.abs(dot), jnp.exp(-max_new))
    done = (numer * (1.0 / (1.0 + jnp.exp(-outgate))) / denom).astype(jnp.bfloat16)
    for peer in range(heads.shape[0]):
        heads[peer] = done
    for copy in copies:
        copy.wait()


def on_chip(*arrays):
    return [pltpu.with_memory_space_constraint(a, pltpu.VMEM) for a in arrays]


def up_body(middle, gain, w_up, taken, out):
    side = lax.axis_index("kv_side")
    rows, columns = w_up.shape
    half = columns // 2
    count = middle.shape[0] // 2
    mine = middle[pl.ds(side * count, count)].reshape(rows, -1).astype(jnp.float32).T
    theirs = middle[pl.ds((1 - side) * count, count)].reshape(rows, -1).astype(jnp.float32).T
    squares = jnp.sum(mine * mine + theirs * theirs, axis=1, keepdims=True)
    gains = taken[rows : rows + 8, :rows].astype(jnp.float32)
    mine = (mine * gain[...]).astype(jnp.bfloat16)
    theirs = (theirs * (gains[0:1] + gains[1:2])).astype(jnp.bfloat16)
    upward = contract(mine, w_up[:, pl.ds(pl.multiple_of(side * half, half), half)], 1, 0)
    upward = upward + contract(theirs, taken[:rows], 1, 0)
    high, low = two_parts(squares)
    upward = upward.astype(jnp.bfloat16)
    peers, tiles, lines, lanes = out.shape
    across = half // lanes
    own = (tiles - 1) // across * lines
    lane = lax.broadcasted_iota(jnp.int32, (lines, lanes), 1)
    for peer in range(peers):
        extra = jnp.zeros((lines, lanes), jnp.float32)
        for part in range(own // lines):
            at = peer * own + part * lines
            for tile in range(across):
                out[peer, part * across + tile] = upward[
                    at : at + lines, tile * lanes : (tile + 1) * lanes
                ]
            extra = jnp.where(lane == 2 * part, high[at : at + lines], extra)
            extra = jnp.where(lane == 2 * part + 1, low[at : at + lines], extra)
        out[peer, tiles - 1] = extra.astype(jnp.bfloat16)


def hidden_body(width, tiles, copies):
    terms = jnp.sum(tiles[...].astype(jnp.float32), axis=0)
    count, lines, lanes = terms.shape
    peers, own, half = copies.shape
    across = half // lanes
    for part in range(own // lines):
        total = terms[count - 1, :, 2 * part : 2 * part + 1]
        total = total + terms[count - 1, :, 2 * part + 1 : 2 * part + 2]
        scale = lax.rsqrt(total / width + EPSILON)
        for tile in range(across):
            upward = jnp.maximum(terms[part * across + tile] * scale, 0.0)
            upward = (upward * upward).astype(jnp.bfloat16)
            for peer in range(peers):
                copies[
                    peer, part * lines : (part + 1) * lines, tile * lanes : (tile + 1) * lanes
                ] = upward


def down_body(hidden, w_down, taken, out):
    side = lax.axis_index("kv_side")
    half = hidden.shape[2]
    count = out.shape[0] // 2
    left = hidden[...].reshape(-1, half)
    mine = contract(left, w_down[pl.ds(pl.multiple_of(side * half, half), half)], 1, 0)
    theirs = contract(left, taken[...], 1, 0)
    shape = (count, *out.shape[1:])
    out[pl.ds((1 - side) * count, count)] = mine.T.astype(jnp.bfloat16).reshape(shape)
    out[pl.ds(side * count, count)] = theirs.T.astype(jnp.bfloat16).reshape(shape)


def in_vmem(body, shape, *operands):
    vmem = pl.BlockSpec(memory_space=pltpu.VMEM)
    return pl.pallas_call(
        body,
        out_shape=pltpu.VMEM(shape, jnp.bfloat16),
        in_specs=[vmem] * len(operands),
        out_specs=vmem,
    )(*on_chip(*operands))


def stage(operands, peers):
    tokens, gain = operands[0], operands[1]
    wi, norm = operands[3], operands[7]
    vmem = pl.BlockSpec(memory_space=pltpu.VMEM)
    out_shape = (
        pltpu.VMEM((peers, *tokens.shape), jnp.bfloat16),
        pltpu.VMEM((8, wi.shape[1]), jnp.bfloat16),
        pltpu.VMEM((norm.shape[0], LANES), jnp.float32),
        pltpu.VMEM(tokens.shape, jnp.float32),
        pltpu.VMEM((8, wi.shape[1]), jnp.bfloat16),
        pltpu.VMEM(gain.shape, jnp.float32),
        pltpu.VMEM(gain.shape, jnp.float32),
        pltpu.VMEM((operands[9].shape[0] + operands[10].shape[0], wi.shape[1]), jnp.bfloat16),
    )
    scratch = [pltpu.VMEM(a.shape, a.dtype) for a in (tokens, *operands[3:9])]
    return pl.pallas_call(
        functools.partial(stage_body, LANES),
        out_shape=out_shape,
        in_specs=[pl.BlockSpec(memory_space=pl.ANY)] * len(operands),
        out_specs=(vmem,) * len(out_shape),
        scratch_shapes=[*scratch, pltpu.SemaphoreType.DMA((len(operands),))],
        name="stage",
    )(*operands)


def memory_step(tiles, cell, aux, gains, w_up, w_down, width):
    peers, own, _ = tiles.shape
    _, key_dim, value_dim = cell.shape
    rows, columns = w_up.shape
    vmem = pl.BlockSpec(memory_space=pltpu.VMEM)
    hbm = pl.BlockSpec(memory_space=pl.ANY)
    return pl.pallas_call(
        functools.partial(memory_body, width),
        out_shape=(
            pltpu.VMEM((peers, own, value_dim), jnp.bfloat16),
            jax.ShapeDtypeStruct(cell.shape, jnp.float32),
            jax.ShapeDtypeStruct((own, key_dim), jnp.float32),
            jax.ShapeDtypeStruct((1, own), jnp.float32),
            pltpu.VMEM((rows + 8, columns // 2), jnp.bfloat16),
            pltpu.VMEM((columns // 2, rows), jnp.bfloat16),
        ),
        in_specs=[vmem] * 4 + [hbm] * 2,
        out_specs=(vmem, hbm, hbm, hbm, vmem, vmem),
        scratch_shapes=[
            pltpu.VMEM(cell.shape, jnp.float32),
            pltpu.VMEM((own, key_dim), jnp.float32),
            pltpu.VMEM((1, own), jnp.float32),
            pltpu.SemaphoreType.DMA((own + 4,)),
        ],
        name="memory",
    )(*on_chip(tiles, cell, aux, gains), w_up, w_down)


def layer(
    tokens,
    gain_in,
    w_query,
    w_key,
    w_value,
    w_outgate,
    w_input_gate,
    w_forget_gate,
    bias_input,
    bias_forget,
    cell_state,
    norm_state,
    max_state,
    w_proj,
    gain_mid,
    w_up,
    w_down,
):
    seqs, own_columns = tokens.shape
    value_dim = cell_state.shape[3]
    tp, kv = lax.axis_size("tp"), lax.axis_size(KV)
    pairs = kv // 2
    half = w_up.shape[1] // 2
    rows = gain_in.shape[0]
    width = rows * kv
    own = seqs // kv
    heads_all = w_input_gate.shape[1]
    swap = [(0, 1), (1, 0)]

    copies, gates, aux, residual, gains, gain_in, gain_mid, w_qk = stage(
        (
            tokens.T,
            gain_in.reshape(1, rows),
            gain_mid.reshape(1, rows),
            w_input_gate.T,
            w_forget_gate.T,
            bias_input.reshape(1, heads_all),
            bias_forget.reshape(1, heads_all),
            norm_state[:, 0],
            max_state.reshape(1, own),
            w_query.T,
            w_key.T,
        ),
        tp,
    )
    terms = in_vmem(
        project_body,
        (kv, own, 4 * LANES),
        exchange(copies, "tp"),
        gain_in,
        gates,
        w_qk,
        w_value,
        w_outgate,
    )
    heads, cell_new, norm_new, max_new, sent_up, sent_down = memory_step(
        exchange(terms, KV), cell_state[:, 0], aux, gains, w_up, w_down, width
    )

    heads = exchange(heads, KV).reshape(seqs, value_dim)
    heads, sent_up, sent_down = lax.optimization_barrier((heads, sent_up, sent_down))
    other_up = lax.ppermute(sent_up, "kv_side", swap)
    shifted = [(i, (i + 2 * (i % 2) - 1) % kv) for i in range(kv)]
    other_down = lax.ppermute(sent_down, KV, shifted)
    branch = contract(w_proj, heads, 0, 1).astype(jnp.bfloat16)
    branch = exchange(branch.reshape(tp, own_columns, seqs), "tp")
    own_middle = residual + jnp.sum(branch.astype(jnp.float32), axis=0)
    own_middle = own_middle.astype(jnp.bfloat16)
    middle = spread(own_middle, ("kv_side", "tp"))
    tiles = 2 * own * half // (8 * LANES) + 1
    upward = in_vmem(up_body, (pairs, tiles, 8, LANES), middle, gain_mid, w_up, other_up)
    upward = exchange(upward, "kv_pair")
    copies = in_vmem(functools.partial(hidden_body, width), (pairs, 2 * own, half), upward)
    copies, other_down = lax.optimization_barrier((copies, other_down))
    hidden = exchange(copies, "kv_pair")
    down = in_vmem(down_body, (2 * tp, own_columns, seqs), hidden, w_down, other_down)
    groups = [
        [k % kv * tp + t for k in (odd, odd + 1) for t in range(tp)] for odd in range(1, kv, 2)
    ]
    down = lax.all_to_all(down, (*KV, "tp"), 0, 0, axis_index_groups=groups, tiled=True)
    mixed = own_middle.astype(jnp.float32) + jnp.sum(down.astype(jnp.float32), axis=0)
    mixed = mixed.astype(jnp.bfloat16).T
    return (mixed, cell_new[:, None], norm_new[:, None], max_new.reshape(own, 1))


def solution(mesh):
    sizes = mesh.devices.shape
    halves = (sizes[0], sizes[1] // 2, 2, sizes[2])
    mesh = jax.sharding.Mesh(mesh.devices.reshape(halves), ("grp", *KV, "tp"))
    in_specs = (
        P("grp", (*KV, "tp")),
        P(KV),
        P(KV, "tp"),
        P(KV, "tp"),
        P(KV, "tp"),
        P(KV, "tp"),
        P(KV, None),
        P(KV, None),
        P(),
        P(),
        P(("grp", *KV), "tp", None, None),
        P(("grp", *KV), "tp", None),
        P(("grp", *KV), "tp"),
        P("tp", KV),
        P(KV),
        P(KV, "tp"),
        P("tp", KV),
    )
    out_specs = (
        P("grp", (*KV, "tp")),
        P(("grp", *KV), "tp", None, None),
        P(("grp", *KV), "tp", None),
        P(("grp", *KV), "tp"),
    )
    return jax.shard_map(layer, mesh=mesh, in_specs=in_specs, out_specs=out_specs, check_vma=False)
```

```python
import functools

import jax
import jax.numpy as jnp
from jax import lax
from jax.experimental import pallas as pl
from jax.experimental.pallas import tpu as pltpu
from jax.sharding import PartitionSpec as P


EPSILON = 1e-06
LANES = 128


KV = ("kv_pair", "kv_side")


def exchange(tiles, axis):
    return lax.all_to_all(tiles, axis, split_axis=0, concat_axis=0, tiled=True)


def spread(value, axis):
    return exchange(jnp.broadcast_to(value, (lax.axis_size(axis), *value.shape)), axis)


def contract(left, right, left_dim, right_dim):
    dims = (((left_dim,), (right_dim,)), ((), ()))
    return lax.dot_general(left, right, dims, preferred_element_type=jnp.float32)


def two_parts(value):
    high = value.astype(jnp.bfloat16).astype(jnp.float32)
    return high, (value - high).astype(jnp.bfloat16).astype(jnp.float32)


def stage_body(
    width, tokens, gain_in, gain_mid, wi, wf, bias_in, bias_forget, norm, top, wq, wk,
    copies, gates, aux, residual, gains, first_gain, second_gain, both_qk,
    own, wi_buf, wf_buf, bias_in_buf, bias_forget_buf, norm_buf, top_buf, sems,
):
    moves = (
        (tokens, own), (gain_in, first_gain), (gain_mid, second_gain), (wi, wi_buf), (wf, wf_buf),
        (bias_in, bias_in_buf), (bias_forget, bias_forget_buf), (norm, norm_buf), (top, top_buf),
        (wq, both_qk.at[pl.ds(0, wq.shape[0])]), (wk, both_qk.at[pl.ds(wq.shape[0], wk.shape[0])]),
    )
    moves = [
        pltpu.make_async_copy(source, target, sems.at[at])
        for at, (source, target) in enumerate(moves)
    ]
    for move in moves:
        move.start()
    for move in moves:
        move.wait()
    head = lax.axis_index("tp")
    value = own[...]
    for peer in range(copies.shape[0]):
        copies[peer] = value
    residual[...] = value.astype(jnp.float32)
    heads, rows = wi_buf.shape
    count, key_dim = norm_buf.shape
    down = lax.broadcasted_iota(jnp.int32, (heads, rows), 0) == head
    line = lax.broadcasted_iota(jnp.int32, (8, rows), 0)
    picked = [
        jnp.sum(jnp.where(down, w[...].astype(jnp.float32), 0.0), axis=0, keepdims=True)
        for w in (wi_buf, wf_buf)
    ]
    both = jnp.where(line == 0, picked[0], jnp.where(line == 1, picked[1], 0.0))
    gates[...] = both.astype(jnp.bfloat16)
    high, low = two_parts(second_gain[...])
    both = jnp.where(line == 0, high, jnp.where(line == 1, low, 0.0))
    gains[...] = both.astype(jnp.bfloat16)
    along = lax.broadcasted_iota(jnp.int32, (1, heads), 1) == head
    place = lax.broadcasted_iota(jnp.int32, (count, width - key_dim), 1)
    first, second = [
        jnp.sum(jnp.where(along, b[...], 0.0), axis=1, keepdims=True)
        for b in (bias_in_buf, bias_forget_buf)
    ]
    eye = lax.broadcasted_iota(jnp.int32, (count, count), 0)
    eye = eye == lax.broadcasted_iota(jnp.int32, (count, count), 1)
    turned = jnp.sum(jnp.where(eye, top_buf[...], 0.0), axis=1, keepdims=True)
    rest = jnp.where(place == 1, first, jnp.where(place == 2, second, 0.0))
    rest = jnp.where(place == 0, turned, rest)
    aux[...] = jnp.concatenate([norm_buf[...], rest], axis=1)


def project_body(tokens, gain, gates, wqk, wv, wo, out):
    wide = tokens[...].reshape(-1, tokens.shape[-1]).astype(jnp.float32).T
    squares = jnp.sum(wide * wide, axis=1, keepdims=True)
    normed = (wide * gain[...]).astype(jnp.bfloat16)
    both = contract(normed, wqk[...], 1, 1)
    values = contract(normed, wv[...], 1, 0)
    outgate = contract(normed, wo[...], 1, 0)
    gate = contract(normed, gates[...], 1, 1)
    lane = lax.broadcasted_iota(jnp.int32, (wide.shape[0], LANES), 1)
    extra = jnp.zeros((wide.shape[0], LANES), jnp.float32)
    for place, value in enumerate((gate[:, 0:1], gate[:, 1:2], squares)):
        high, low = two_parts(value)
        extra = jnp.where(lane == place, high, extra)
        extra = jnp.where(lane == place + 3, low, extra)
    peers, own, _ = out.shape
    at = 0
    for piece in (both, values, outgate, extra):
        piece = piece.astype(jnp.bfloat16)
        for peer in range(peers):
            out[peer, :, at : at + LANES] = piece[peer * own : (peer + 1) * own]
        at += LANES


def memory_body(
    width, tiles, cell, aux, gains, w_up, w_down,
    heads, cell_out, norm_out, top_out, sent_up, sent_down, cell_new, norm_buf, top_buf, sems,
):
    rows, columns = w_up.shape
    half = columns // 2
    at = pl.multiple_of((1 - lax.axis_index("kv_side")) * half, half)
    last = sems.shape[0] - 1
    copies = [
        pltpu.make_async_copy(
            w_up.at[:, pl.ds(at, half)], sent_up.at[pl.ds(0, rows)], sems.at[last - 1]
        ),
        pltpu.make_async_copy(w_down.at[pl.ds(at, half)], sent_down, sems.at[last]),
    ]
    for copy in copies:
        copy.start()
    sent_up[rows:, :rows] = gains[...]
    sent_up[rows:, rows:] = jnp.zeros((8, half - rows), jnp.bfloat16)
    own, key_dim, _ = cell.shape
    terms = jnp.sum(tiles[...].astype(jnp.float32), axis=0)
    extra = terms[:, 3 * LANES :]
    extra = extra[:, 0:3] + extra[:, 3:6]
    scale = lax.rsqrt(extra[:, 2:3] / width + EPSILON)
    side = aux[...]
    norm, top = side[:, :key_dim], side[:, key_dim : key_dim + 1]
    log_input = extra[:, 0:1] * scale + side[:, key_dim + 1 : key_dim + 2]
    forget = extra[:, 1:2] * scale + side[:, key_dim + 2 : key_dim + 3]
    log_forget = jnp.minimum(forget, 0.0) - jnp.log1p(jnp.exp(-jnp.abs(forget)))
    log_keep = log_forget + top
    max_new = jnp.maximum(log_keep, log_input)
    keep = jnp.exp(log_keep - max_new)
    write = jnp.exp(log_input - max_new)
    top_buf[...] = jnp.broadcast_to(max_new, (own, LANES)).T[0:1]
    lane = lax.broadcasted_iota(jnp.int32, (own, LANES), 1)
    is_query = lane < key_dim
    both = terms[:, :LANES] * jnp.where(is_query, scale * key_dim ** (-0.5), scale * write)
    values = terms[:, LANES : 2 * LANES] * scale
    outgate = terms[:, 2 * LANES : 3 * LANES] * scale
    turned = jnp.concatenate([both] * (LANES // own), axis=0).T
    norm_new = keep * norm + both[:, key_dim:]
    norm_buf[...] = norm_new
    for buf, target, sem in ((top_buf, top_out, own), (norm_buf, norm_out, own + 1)):
        copies.append(pltpu.make_async_copy(buf, target, sems.at[sem]))
        copies[-1].start()
    rows = []
    for s in range(own):
        fresh = keep[s : s + 1] * cell[s] + turned[key_dim:, s : s + 1] * values[s : s + 1]
        cell_new[s] = fresh
        copies.append(pltpu.make_async_copy(cell_new.at[s], cell_out.at[s], sems.at[s]))
        copies[-1].start()
        rows.append(jnp.sum(turned[:key_dim, s : s + 1] * fresh, axis=0, keepdims=True))
    numer = jnp.concatenate(rows, axis=0)
    dot = jnp.sum(both[:, :key_dim] * norm_new, axis=1, keepdims=True)
    denom = jnp.maximum(jnp.abs(dot), jnp.exp(-max_new))
    done = (numer * (1.0 / (1.0 + jnp.exp(-outgate))) / denom).astype(jnp.bfloat16)
    for peer in range(heads.shape[0]):
        heads[peer] = done
    for copy in copies:
        copy.wait()


def on_chip(*arrays):
    return [pltpu.with_memory_space_constraint(a, pltpu.VMEM) for a in arrays]


def up_body(middle, gain, w_up, taken, out):
    side = lax.axis_index("kv_side")
    rows, columns = w_up.shape
    half = columns // 2
    count = middle.shape[0] // 2
    mine = middle[pl.ds(side * count, count)].reshape(rows, -1).astype(jnp.float32).T
    theirs = middle[pl.ds((1 - side) * count, count)].reshape(rows, -1).astype(jnp.float32).T
    squares = jnp.sum(mine * mine + theirs * theirs, axis=1, keepdims=True)
    gains = taken[rows : rows + 8, :rows].astype(jnp.float32)
    mine = (mine * gain[...]).astype(jnp.bfloat16)
    theirs = (theirs * (gains[0:1] + gains[1:2])).astype(jnp.bfloat16)
    upward = contract(mine, w_up[:, pl.ds(pl.multiple_of(side * half, half), half)], 1, 0)
    upward = upward + contract(theirs, taken[:rows], 1, 0)
    high, low = two_parts(squares)
    upward = upward.astype(jnp.bfloat16)
    peers, tiles, lines, lanes = out.shape
    across = half // lanes
    own = (tiles - 1) // across * lines
    lane = lax.broadcasted_iota(jnp.int32, (lines, lanes), 1)
    for peer in range(peers):
        extra = jnp.zeros((lines, lanes), jnp.float32)
        for part in range(own // lines):
            at = peer * own + part * lines
            for tile in range(across):
                out[peer, part * across + tile] = upward[
                    at : at + lines, tile * lanes : (tile + 1) * lanes
                ]
            extra = jnp.where(lane == 2 * part, high[at : at + lines], extra)
            extra = jnp.where(lane == 2 * part + 1, low[at : at + lines], extra)
        out[peer, tiles - 1] = extra.astype(jnp.bfloat16)


def hidden_body(width, tiles, copies):
    terms = jnp.sum(tiles[...].astype(jnp.float32), axis=0)
    count, lines, lanes = terms.shape
    peers, own, half = copies.shape
    across = half // lanes
    for part in range(own // lines):
        total = terms[count - 1, :, 2 * part : 2 * part + 1]
        total = total + terms[count - 1, :, 2 * part + 1 : 2 * part + 2]
        scale = lax.rsqrt(total / width + EPSILON)
        for tile in range(across):
            upward = jnp.maximum(terms[part * across + tile] * scale, 0.0)
            upward = (upward * upward).astype(jnp.bfloat16)
            for peer in range(peers):
                copies[
                    peer, part * lines : (part + 1) * lines, tile * lanes : (tile + 1) * lanes
                ] = upward


def down_body(hidden, w_down, taken, out):
    side = lax.axis_index("kv_side")
    half = hidden.shape[2]
    count = out.shape[0] // 2
    left = hidden[...].reshape(-1, half)
    mine = contract(left, w_down[pl.ds(pl.multiple_of(side * half, half), half)], 1, 0)
    theirs = contract(left, taken[...], 1, 0)
    shape = (count, *out.shape[1:])
    out[pl.ds(side * count, count)] = mine.T.astype(jnp.bfloat16).reshape(shape)
    out[pl.ds((1 - side) * count, count)] = theirs.T.astype(jnp.bfloat16).reshape(shape)


def in_vmem(body, shape, *operands):
    vmem = pl.BlockSpec(memory_space=pltpu.VMEM)
    return pl.pallas_call(
        body,
        out_shape=pltpu.VMEM(shape, jnp.bfloat16),
        in_specs=[vmem] * len(operands),
        out_specs=vmem,
    )(*on_chip(*operands))


def stage(operands, peers):
    tokens, gain = operands[0], operands[1]
    wi, norm = operands[3], operands[7]
    vmem = pl.BlockSpec(memory_space=pltpu.VMEM)
    out_shape = (
        pltpu.VMEM((peers, *tokens.shape), jnp.bfloat16),
        pltpu.VMEM((8, wi.shape[1]), jnp.bfloat16),
        pltpu.VMEM((norm.shape[0], LANES), jnp.float32),
        pltpu.VMEM(tokens.shape, jnp.float32),
        pltpu.VMEM((8, wi.shape[1]), jnp.bfloat16),
        pltpu.VMEM(gain.shape, jnp.float32),
        pltpu.VMEM(gain.shape, jnp.float32),
        pltpu.VMEM((operands[9].shape[0] + operands[10].shape[0], wi.shape[1]), jnp.bfloat16),
    )
    scratch = [pltpu.VMEM(a.shape, a.dtype) for a in (tokens, *operands[3:9])]
    return pl.pallas_call(
        functools.partial(stage_body, LANES),
        out_shape=out_shape,
        in_specs=[pl.BlockSpec(memory_space=pl.ANY)] * len(operands),
        out_specs=(vmem,) * len(out_shape),
        scratch_shapes=[*scratch, pltpu.SemaphoreType.DMA((len(operands),))],
        name="stage",
    )(*operands)


def memory_step(tiles, cell, aux, gains, w_up, w_down, width):
    peers, own, _ = tiles.shape
    _, key_dim, value_dim = cell.shape
    rows, columns = w_up.shape
    vmem = pl.BlockSpec(memory_space=pltpu.VMEM)
    hbm = pl.BlockSpec(memory_space=pl.ANY)
    return pl.pallas_call(
        functools.partial(memory_body, width),
        out_shape=(
            pltpu.VMEM((peers, own, value_dim), jnp.bfloat16),
            jax.ShapeDtypeStruct(cell.shape, jnp.float32),
            jax.ShapeDtypeStruct((own, key_dim), jnp.float32),
            jax.ShapeDtypeStruct((1, own), jnp.float32),
            pltpu.VMEM((rows + 8, columns // 2), jnp.bfloat16),
            pltpu.VMEM((columns // 2, rows), jnp.bfloat16),
        ),
        in_specs=[vmem] * 4 + [hbm] * 2,
        out_specs=(vmem, hbm, hbm, hbm, vmem, vmem),
        scratch_shapes=[
            pltpu.VMEM(cell.shape, jnp.float32),
            pltpu.VMEM((own, key_dim), jnp.float32),
            pltpu.VMEM((1, own), jnp.float32),
            pltpu.SemaphoreType.DMA((own + 4,)),
        ],
        name="memory",
    )(*on_chip(tiles, cell, aux, gains), w_up, w_down)


def layer(
    tokens,
    gain_in,
    w_query,
    w_key,
    w_value,
    w_outgate,
    w_input_gate,
    w_forget_gate,
    bias_input,
    bias_forget,
    cell_state,
    norm_state,
    max_state,
    w_proj,
    gain_mid,
    w_up,
    w_down,
):
    seqs, own_columns = tokens.shape
    value_dim = cell_state.shape[3]
    tp, kv = lax.axis_size("tp"), lax.axis_size(KV)
    pairs = kv // 2
    half = w_up.shape[1] // 2
    rows = gain_in.shape[0]
    width = rows * kv
    own = seqs // kv
    heads_all = w_input_gate.shape[1]
    swap = [(0, 1), (1, 0)]

    copies, gates, aux, residual, gains, gain_in, gain_mid, w_qk = stage(
        (
            tokens.T,
            gain_in.reshape(1, rows),
            gain_mid.reshape(1, rows),
            w_input_gate.T,
            w_forget_gate.T,
            bias_input.reshape(1, heads_all),
            bias_forget.reshape(1, heads_all),
            norm_state[:, 0],
            max_state.reshape(1, own),
            w_query.T,
            w_key.T,
        ),
        tp,
    )
    terms = in_vmem(
        project_body,
        (kv, own, 4 * LANES),
        exchange(copies, "tp"),
        gain_in,
        gates,
        w_qk,
        w_value,
        w_outgate,
    )
    heads, cell_new, norm_new, max_new, sent_up, sent_down = memory_step(
        exchange(terms, KV), cell_state[:, 0], aux, gains, w_up, w_down, width
    )

    heads = exchange(heads, KV)
    other_up = lax.ppermute(sent_up, "kv_side", swap)
    other_down = lax.ppermute(sent_down, "kv_side", swap)

    heads = heads.reshape(seqs, value_dim)
    branch = contract(w_proj, heads, 0, 1).astype(jnp.bfloat16)
    branch = exchange(branch.reshape(tp, own_columns, seqs), "tp")
    own_middle = residual + jnp.sum(branch.astype(jnp.float32), axis=0)
    own_middle = own_middle.astype(jnp.bfloat16)
    own_middle, other_up, other_down = lax.optimization_barrier((own_middle, other_up, other_down))
    middle = spread(own_middle, ("kv_side", "tp"))
    tiles = 2 * own * half // (8 * LANES) + 1
    upward = in_vmem(up_body, (pairs, tiles, 8, LANES), middle, gain_mid, w_up, other_up)
    upward = exchange(upward, "kv_pair")
    copies = in_vmem(functools.partial(hidden_body, width), (pairs, 2 * own, half), upward)
    hidden = exchange(copies, "kv_pair")
    down = in_vmem(down_body, (2 * tp, own_columns, seqs), hidden, w_down, other_down)
    down = exchange(down, ("kv_side", "tp"))
    mixed = own_middle.astype(jnp.float32) + jnp.sum(down.astype(jnp.float32), axis=0)
    mixed = mixed.astype(jnp.bfloat16).T
    return (mixed, cell_new[:, None], norm_new[:, None], max_new.reshape(own, 1))


def solution(mesh):
    sizes = mesh.devices.shape
    halves = (sizes[0], sizes[1] // 2, 2, sizes[2])
    mesh = jax.sharding.Mesh(mesh.devices.reshape(halves), ("grp", *KV, "tp"))
    in_specs = (
        P("grp", (*KV, "tp")),
        P(KV),
        P(KV, "tp"),
        P(KV, "tp"),
        P(KV, "tp"),
        P(KV, "tp"),
        P(KV, None),
        P(KV, None),
        P(),
        P(),
        P(("grp", *KV), "tp", None, None),
        P(("grp", *KV), "tp", None),
        P(("grp", *KV), "tp"),
        P("tp", KV),
        P(KV),
        P(KV, "tp"),
        P("tp", KV),
    )
    out_specs = (
        P("grp", (*KV, "tp")),
        P(("grp", *KV), "tp", None, None),
        P(("grp", *KV), "tp", None),
        P(("grp", *KV), "tp"),
    )
    return jax.shard_map(layer, mesh=mesh, in_specs=in_specs, out_specs=out_specs, check_vma=False)
```

```python
import functools

import jax
import jax.numpy as jnp
from jax import lax
from jax.experimental import pallas as pl
from jax.experimental.pallas import tpu as pltpu
from jax.sharding import PartitionSpec as P


EPSILON = 1e-06
LANES = 128


KV = ("kv_pair", "kv_side")


def exchange(tiles, axis):
    return lax.all_to_all(tiles, axis, split_axis=0, concat_axis=0, tiled=True)


def spread(value, axis):
    return exchange(jnp.broadcast_to(value, (lax.axis_size(axis), *value.shape)), axis)


def contract(left, right, left_dim, right_dim):
    dims = (((left_dim,), (right_dim,)), ((), ()))
    return lax.dot_general(left, right, dims, preferred_element_type=jnp.float32)


def two_parts(value):
    high = value.astype(jnp.bfloat16).astype(jnp.float32)
    return high, (value - high).astype(jnp.bfloat16).astype(jnp.float32)


def stage_body(
    width, tokens, gain_in, gain_mid, wi, wf, bias_in, bias_forget, norm, top, wq, wk,
    copies, gates, aux, residual, gains, first_gain, second_gain, both_qk,
    own, wi_buf, wf_buf, bias_in_buf, bias_forget_buf, norm_buf, top_buf, sems,
):
    moves = (
        (tokens, own), (gain_in, first_gain), (gain_mid, second_gain), (wi, wi_buf), (wf, wf_buf),
        (bias_in, bias_in_buf), (bias_forget, bias_forget_buf), (norm, norm_buf), (top, top_buf),
        (wq, both_qk.at[pl.ds(0, wq.shape[0])]), (wk, both_qk.at[pl.ds(wq.shape[0], wk.shape[0])]),
    )
    moves = [
        pltpu.make_async_copy(source, target, sems.at[at])
        for at, (source, target) in enumerate(moves)
    ]
    for move in moves:
        move.start()
    for move in moves:
        move.wait()
    head = lax.axis_index("tp")
    value = own[...]
    for peer in range(copies.shape[0]):
        copies[peer] = value
    residual[...] = value.astype(jnp.float32)
    heads, rows = wi_buf.shape
    count, key_dim = norm_buf.shape
    down = lax.broadcasted_iota(jnp.int32, (heads, rows), 0) == head
    line = lax.broadcasted_iota(jnp.int32, (8, rows), 0)
    picked = [
        jnp.sum(jnp.where(down, w[...].astype(jnp.float32), 0.0), axis=0, keepdims=True)
        for w in (wi_buf, wf_buf)
    ]
    both = jnp.where(line == 0, picked[0], jnp.where(line == 1, picked[1], 0.0))
    gates[...] = both.astype(jnp.bfloat16)
    high, low = two_parts(second_gain[...])
    both = jnp.where(line == 0, high, jnp.where(line == 1, low, 0.0))
    gains[...] = both.astype(jnp.bfloat16)
    along = lax.broadcasted_iota(jnp.int32, (1, heads), 1) == head
    place = lax.broadcasted_iota(jnp.int32, (count, width - key_dim), 1)
    first, second = [
        jnp.sum(jnp.where(along, b[...], 0.0), axis=1, keepdims=True)
        for b in (bias_in_buf, bias_forget_buf)
    ]
    eye = lax.broadcasted_iota(jnp.int32, (count, count), 0)
    eye = eye == lax.broadcasted_iota(jnp.int32, (count, count), 1)
    turned = jnp.sum(jnp.where(eye, top_buf[...], 0.0), axis=1, keepdims=True)
    rest = jnp.where(place == 1, first, jnp.where(place == 2, second, 0.0))
    rest = jnp.where(place == 0, turned, rest)
    aux[...] = jnp.concatenate([norm_buf[...], rest], axis=1)


def project_body(tokens, gain, gates, wqk, wv, wo, out):
    wide = tokens[...].reshape(-1, tokens.shape[-1]).astype(jnp.float32).T
    squares = jnp.sum(wide * wide, axis=1, keepdims=True)
    normed = (wide * gain[...]).astype(jnp.bfloat16)
    both = contract(normed, wqk[...], 1, 1)
    values = contract(normed, wv[...], 1, 0)
    outgate = contract(normed, wo[...], 1, 0)
    gate = contract(normed, gates[...], 1, 1)
    lane = lax.broadcasted_iota(jnp.int32, (wide.shape[0], LANES), 1)
    extra = jnp.zeros((wide.shape[0], LANES), jnp.float32)
    for place, value in enumerate((gate[:, 0:1], gate[:, 1:2], squares)):
        high, low = two_parts(value)
        extra = jnp.where(lane == place, high, extra)
        extra = jnp.where(lane == place + 3, low, extra)
    peers, own, _ = out.shape
    at = 0
    for piece in (both, values, outgate, extra):
        piece = piece.astype(jnp.bfloat16)
        for peer in range(peers):
            out[peer, :, at : at + LANES] = piece[peer * own : (peer + 1) * own]
        at += LANES


def memory_body(
    width, tiles, cell, aux, gains, w_up, w_down,
    heads_out, cell_out, norm_out, top_out, sent_up, sent_down,
    heads, cell_new, norm_buf, top_buf, sems,
):
    rows, columns = w_up.shape
    half = columns // 2
    at = pl.multiple_of((1 - lax.axis_index("kv_side")) * half, half)
    last = sems.shape[0] - 2
    copies = [
        pltpu.make_async_copy(
            w_up.at[:, pl.ds(at, half)], sent_up.at[pl.ds(0, rows)], sems.at[last - 1]
        ),
        pltpu.make_async_copy(w_down.at[pl.ds(at, half)], sent_down, sems.at[last]),
    ]
    for copy in copies:
        copy.start()
    sent_up[rows:, :rows] = gains[...]
    sent_up[rows:, rows:] = jnp.zeros((8, half - rows), jnp.bfloat16)
    own, key_dim, _ = cell.shape
    terms = jnp.sum(tiles[...].astype(jnp.float32), axis=0)
    extra = terms[:, 3 * LANES :]
    extra = extra[:, 0:3] + extra[:, 3:6]
    scale = lax.rsqrt(extra[:, 2:3] / width + EPSILON)
    side = aux[...]
    norm, top = side[:, :key_dim], side[:, key_dim : key_dim + 1]
    log_input = extra[:, 0:1] * scale + side[:, key_dim + 1 : key_dim + 2]
    forget = extra[:, 1:2] * scale + side[:, key_dim + 2 : key_dim + 3]
    log_forget = jnp.minimum(forget, 0.0) - jnp.log1p(jnp.exp(-jnp.abs(forget)))
    log_keep = log_forget + top
    max_new = jnp.maximum(log_keep, log_input)
    keep = jnp.exp(log_keep - max_new)
    write = jnp.exp(log_input - max_new)
    top_buf[...] = jnp.broadcast_to(max_new, (own, LANES)).T[0:1]
    lane = lax.broadcasted_iota(jnp.int32, (own, LANES), 1)
    is_query = lane < key_dim
    both = terms[:, :LANES] * jnp.where(is_query, scale * key_dim ** (-0.5), scale * write)
    values = terms[:, LANES : 2 * LANES] * scale
    outgate = terms[:, 2 * LANES : 3 * LANES] * scale
    turned = jnp.concatenate([both] * (LANES // own), axis=0).T
    norm_new = keep * norm + both[:, key_dim:]
    norm_buf[...] = norm_new
    for buf, target, sem in ((top_buf, top_out, own), (norm_buf, norm_out, own + 1)):
        copies.append(pltpu.make_async_copy(buf, target, sems.at[sem]))
        copies[-1].start()
    rows = []
    for s in range(own):
        fresh = keep[s : s + 1] * cell[s] + turned[key_dim:, s : s + 1] * values[s : s + 1]
        cell_new[s] = fresh
        copies.append(pltpu.make_async_copy(cell_new.at[s], cell_out.at[s], sems.at[s]))
        copies[-1].start()
        rows.append(jnp.sum(turned[:key_dim, s : s + 1] * fresh, axis=0, keepdims=True))
    numer = jnp.concatenate(rows, axis=0)
    dot = jnp.sum(both[:, :key_dim] * norm_new, axis=1, keepdims=True)
    denom = jnp.maximum(jnp.abs(dot), jnp.exp(-max_new))
    done = (numer * (1.0 / (1.0 + jnp.exp(-outgate))) / denom).astype(jnp.bfloat16)
    for peer in range(heads.shape[0]):
        heads[peer] = done
    copies.append(pltpu.make_async_copy(heads, heads_out, sems.at[last + 1]))
    copies[-1].start()
    for copy in copies:
        copy.wait()


def on_chip(*arrays):
    return [pltpu.with_memory_space_constraint(a, pltpu.VMEM) for a in arrays]


def up_body(middle, gain, w_up, taken, out):
    side = lax.axis_index("kv_side")
    rows, columns = w_up.shape
    half = columns // 2
    count = middle.shape[0] // 2
    mine = middle[pl.ds(side * count, count)].reshape(rows, -1).astype(jnp.float32).T
    theirs = middle[pl.ds((1 - side) * count, count)].reshape(rows, -1).astype(jnp.float32).T
    squares = jnp.sum(mine * mine + theirs * theirs, axis=1, keepdims=True)
    gains = taken[rows : rows + 8, :rows].astype(jnp.float32)
    mine = (mine * gain[...]).astype(jnp.bfloat16)
    theirs = (theirs * (gains[0:1] + gains[1:2])).astype(jnp.bfloat16)
    upward = contract(mine, w_up[:, pl.ds(pl.multiple_of(side * half, half), half)], 1, 0)
    upward = upward + contract(theirs, taken[:rows], 1, 0)
    high, low = two_parts(squares)
    upward = upward.astype(jnp.bfloat16)
    peers, tiles, lines, lanes = out.shape
    across = half // lanes
    own = (tiles - 1) // across * lines
    lane = lax.broadcasted_iota(jnp.int32, (lines, lanes), 1)
    for peer in range(peers):
        extra = jnp.zeros((lines, lanes), jnp.float32)
        for part in range(own // lines):
            at = peer * own + part * lines
            for tile in range(across):
                out[peer, part * across + tile] = upward[
                    at : at + lines, tile * lanes : (tile + 1) * lanes
                ]
            extra = jnp.where(lane == 2 * part, high[at : at + lines], extra)
            extra = jnp.where(lane == 2 * part + 1, low[at : at + lines], extra)
        out[peer, tiles - 1] = extra.astype(jnp.bfloat16)


def hidden_body(width, tiles, copies):
    terms = jnp.sum(tiles[...].astype(jnp.float32), axis=0)
    count, lines, lanes = terms.shape
    peers, own, half = copies.shape
    across = half // lanes
    for part in range(own // lines):
        total = terms[count - 1, :, 2 * part : 2 * part + 1]
        total = total + terms[count - 1, :, 2 * part + 1 : 2 * part + 2]
        scale = lax.rsqrt(total / width + EPSILON)
        for tile in range(across):
            upward = jnp.maximum(terms[part * across + tile] * scale, 0.0)
            upward = (upward * upward).astype(jnp.bfloat16)
            for peer in range(peers):
                copies[
                    peer, part * lines : (part + 1) * lines, tile * lanes : (tile + 1) * lanes
                ] = upward


def down_body(hidden, w_down, taken, out):
    side = lax.axis_index("kv_side")
    half = hidden.shape[2]
    count = out.shape[0] // 2
    left = hidden[...].reshape(-1, half)
    mine = contract(left, w_down[pl.ds(pl.multiple_of(side * half, half), half)], 1, 0)
    theirs = contract(left, taken[...], 1, 0)
    shape = (count, *out.shape[1:])
    out[pl.ds(side * count, count)] = mine.T.astype(jnp.bfloat16).reshape(shape)
    out[pl.ds((1 - side) * count, count)] = theirs.T.astype(jnp.bfloat16).reshape(shape)


def in_vmem(body, shape, *operands):
    vmem = pl.BlockSpec(memory_space=pltpu.VMEM)
    return pl.pallas_call(
        body,
        out_shape=pltpu.VMEM(shape, jnp.bfloat16),
        in_specs=[vmem] * len(operands),
        out_specs=vmem,
    )(*on_chip(*operands))


def stage(operands, peers):
    tokens, gain = operands[0], operands[1]
    wi, norm = operands[3], operands[7]
    vmem = pl.BlockSpec(memory_space=pltpu.VMEM)
    out_shape = (
        pltpu.VMEM((peers, *tokens.shape), jnp.bfloat16),
        pltpu.VMEM((8, wi.shape[1]), jnp.bfloat16),
        pltpu.VMEM((norm.shape[0], LANES), jnp.float32),
        pltpu.VMEM(tokens.shape, jnp.float32),
        pltpu.VMEM((8, wi.shape[1]), jnp.bfloat16),
        pltpu.VMEM(gain.shape, jnp.float32),
        pltpu.VMEM(gain.shape, jnp.float32),
        pltpu.VMEM((operands[9].shape[0] + operands[10].shape[0], wi.shape[1]), jnp.bfloat16),
    )
    scratch = [pltpu.VMEM(a.shape, a.dtype) for a in (tokens, *operands[3:9])]
    return pl.pallas_call(
        functools.partial(stage_body, LANES),
        out_shape=out_shape,
        in_specs=[pl.BlockSpec(memory_space=pl.ANY)] * len(operands),
        out_specs=(vmem,) * len(out_shape),
        scratch_shapes=[*scratch, pltpu.SemaphoreType.DMA((len(operands),))],
        name="stage",
    )(*operands)


def memory_step(tiles, cell, aux, gains, w_up, w_down, width):
    peers, own, _ = tiles.shape
    _, key_dim, value_dim = cell.shape
    rows, columns = w_up.shape
    vmem = pl.BlockSpec(memory_space=pltpu.VMEM)
    hbm = pl.BlockSpec(memory_space=pl.ANY)
    return pl.pallas_call(
        functools.partial(memory_body, width),
        out_shape=(
            jax.ShapeDtypeStruct((peers, own, value_dim), jnp.bfloat16),
            jax.ShapeDtypeStruct(cell.shape, jnp.float32),
            jax.ShapeDtypeStruct((own, key_dim), jnp.float32),
            jax.ShapeDtypeStruct((1, own), jnp.float32),
            pltpu.VMEM((rows + 8, columns // 2), jnp.bfloat16),
            pltpu.VMEM((columns // 2, rows), jnp.bfloat16),
        ),
        in_specs=[vmem] * 4 + [hbm] * 2,
        out_specs=(hbm, hbm, hbm, hbm, vmem, vmem),
        scratch_shapes=[
            pltpu.VMEM((peers, own, value_dim), jnp.bfloat16),
            pltpu.VMEM(cell.shape, jnp.float32),
            pltpu.VMEM((own, key_dim), jnp.float32),
            pltpu.VMEM((1, own), jnp.float32),
            pltpu.SemaphoreType.DMA((own + 5,)),
        ],
        name="memory",
    )(*on_chip(tiles, cell, aux, gains), w_up, w_down)


def layer(
    tokens,
    gain_in,
    w_query,
    w_key,
    w_value,
    w_outgate,
    w_input_gate,
    w_forget_gate,
    bias_input,
    bias_forget,
    cell_state,
    norm_state,
    max_state,
    w_proj,
    gain_mid,
    w_up,
    w_down,
):
    seqs, own_columns = tokens.shape
    value_dim = cell_state.shape[3]
    tp, kv = lax.axis_size("tp"), lax.axis_size(KV)
    pairs = kv // 2
    half = w_up.shape[1] // 2
    rows = gain_in.shape[0]
    width = rows * kv
    own = seqs // kv
    heads_all = w_input_gate.shape[1]
    swap = [(0, 1), (1, 0)]

    copies, gates, aux, residual, gains, gain_in, gain_mid, w_qk = stage(
        (
            tokens.T,
            gain_in.reshape(1, rows),
            gain_mid.reshape(1, rows),
            w_input_gate.T,
            w_forget_gate.T,
            bias_input.reshape(1, heads_all),
            bias_forget.reshape(1, heads_all),
            norm_state[:, 0],
            max_state.reshape(1, own),
            w_query.T,
            w_key.T,
        ),
        tp,
    )
    terms = in_vmem(
        project_body,
        (kv, own, 4 * LANES),
        exchange(copies, "tp"),
        gain_in,
        gates,
        w_qk,
        w_value,
        w_outgate,
    )
    heads, cell_new, norm_new, max_new, sent_up, sent_down = memory_step(
        exchange(terms, KV), cell_state[:, 0], aux, gains, w_up, w_down, width
    )

    heads = exchange(heads, KV)
    other_up = lax.ppermute(sent_up, "kv_side", swap)
    other_down = lax.ppermute(sent_down, "kv_side", swap)

    heads = heads.reshape(seqs, value_dim)
    branch = contract(w_proj, heads, 0, 1).astype(jnp.bfloat16)
    branch = exchange(branch.reshape(tp, own_columns, seqs), "tp")
    own_middle = residual + jnp.sum(branch.astype(jnp.float32), axis=0)
    own_middle = own_middle.astype(jnp.bfloat16)
    own_middle, other_up, other_down = lax.optimization_barrier((own_middle, other_up, other_down))
    middle = spread(own_middle, ("kv_side", "tp"))
    tiles = 2 * own * half // (8 * LANES) + 1
    upward = in_vmem(up_body, (pairs, tiles, 8, LANES), middle, gain_mid, w_up, other_up)
    upward = exchange(upward, "kv_pair")
    copies = in_vmem(functools.partial(hidden_body, width), (pairs, 2 * own, half), upward)
    hidden = exchange(copies, "kv_pair")
    down = in_vmem(down_body, (2 * tp, own_columns, seqs), hidden, w_down, other_down)
    down = exchange(down, ("kv_side", "tp"))
    mixed = own_middle.astype(jnp.float32) + jnp.sum(down.astype(jnp.float32), axis=0)
    mixed = mixed.astype(jnp.bfloat16).T
    return (mixed, cell_new[:, None], norm_new[:, None], max_new.reshape(own, 1))


def solution(mesh):
    sizes = mesh.devices.shape
    halves = (sizes[0], sizes[1] // 2, 2, sizes[2])
    mesh = jax.sharding.Mesh(mesh.devices.reshape(halves), ("grp", *KV, "tp"))
    in_specs = (
        P("grp", (*KV, "tp")),
        P(KV),
        P(KV, "tp"),
        P(KV, "tp"),
        P(KV, "tp"),
        P(KV, "tp"),
        P(KV, None),
        P(KV, None),
        P(),
        P(),
        P(("grp", *KV), "tp", None, None),
        P(("grp", *KV), "tp", None),
        P(("grp", *KV), "tp"),
        P("tp", KV),
        P(KV),
        P(KV, "tp"),
        P("tp", KV),
    )
    out_specs = (
        P("grp", (*KV, "tp")),
        P(("grp", *KV), "tp", None, None),
        P(("grp", *KV), "tp", None),
        P(("grp", *KV), "tp"),
    )
    return jax.shard_map(layer, mesh=mesh, in_specs=in_specs, out_specs=out_specs, check_vma=False)
```
